128 devices in a mesh: sp: 32 (over z, y, core), tp: 4 (over x).
Axes of the slice: x: 4, y: 4, z: 4, core: 2. Of those that a mesh axis runs over, the one named last changes fastest.
Arguments:
- tokens: bfloat16 [16384, 2048], P(('sp', 'tp')), may hold values from -6 to 6
- queries: bfloat16 [16384, 1024], P('sp', 'tp'), may hold values from -160 to 160
- keys: bfloat16 [16384, 1024], P('sp', 'tp'), may hold values from -8 to 8
- values: bfloat16 [16384, 1024], P('sp', 'tp'), may hold values from -6 to 6
- lambdas: float32 [8], P('tp'), may hold values from 0.3 to 0.8
- head_gain: float32 [128], replicated, may hold values from 0.1 to 1.9
- out_weight: bfloat16 [1024, 2048], replicated, may hold values from -0.1875 to 0.1875
- mixer_gain: float32 [2048], replicated, may hold values from 0.1 to 1.9
- up_weight: bfloat16 [2048, 4096], P('sp', 'tp'), may hold values from -0.125 to 0.125
- down_weight: bfloat16 [4096, 2048], P('tp', 'sp'), may hold values from -0.09375 to 0.09375
Outputs:
- result: bfloat16 [16384, 2048], P(('sp', 'tp'))
The draws below stay inside these ranges and needn't reach their ends.
All inputs are finite; a program needn't handle non-finite values.
Results may differ from the reference program's by a relative error of at most 0.02.
Values may be sent and summed in bfloat16 or wider, within the bound.
A program may use at most 128 MiB of HBM per device.

```python
import math
import jax
import jax.numpy as jnp
from jax import lax

D = 2048
HEADS = 8
DQK = 64
DV = 128
ATTN = 1024
FF = 4096
TOKENS = 16384


def drawn(key):
    base = jax.random.normal(jax.random.fold_in(key, 11), (TOKENS, HEADS * 2 * DQK), jnp.float32) * 1.3
    base = jnp.clip(base, -7.8, 7.8)
    return base


def draw_keys(key, part):
    base = drawn(key)
    return base.astype(jnp.bfloat16)


def draw_queries(key, part):
    own = jax.random.normal(jax.random.fold_in(key, 21), (TOKENS, HEADS * 2 * DQK), jnp.float32) * 1.3
    own = jnp.clip(own, -7.8, 7.8)
    return own.astype(jnp.bfloat16)


def steps_of(own_key, shape, pieces, least, top_value):
    loudness = 1.0
    for position, blocks in pieces:
        steps = jax.random.uniform(jax.random.fold_in(jax.random.fold_in(own_key, 6), position), (blocks,), jnp.float32, least / len(pieces), top_value / len(pieces))
        loudness = loudness * jnp.repeat(jnp.exp(steps), shape[position] // blocks).reshape((-1,) + (1,) * (len(shape) - 1 - position))
    return loudness


def bell_draw(key, dims, width, most, cuts=(), kind=jnp.bfloat16):
    entries = jax.random.normal(key, dims, jnp.float32) * width
    if len(cuts) > 0:
        entries = steps_of(key, dims, cuts, -0.22, 0.18) * entries
    return jnp.clip(entries, min=-most, max=most).astype(kind)


def setup_inputs(seed: int = 0) -> dict:
    splits = jax.random.split(jax.random.key(seed), 11)
    tokens = bell_draw(splits[0], (TOKENS, D), 1.0, 6.0, ((0, 128),))
    queries = draw_queries(jax.random.fold_in(splits[10], 71), 0)
    keys = draw_keys(jax.random.fold_in(splits[10], 71), 0)
    values = bell_draw(splits[3], (TOKENS, ATTN), 1.0, 6.0, ((0, 32), (1, 4)))
    lambdas = jnp.clip(0.3 + 0.5 * jax.random.uniform(splits[4], (HEADS,), jnp.float32) ** steps_of(splits[4], (HEADS,), ((0, 4),), -0.2, 0.2), 0.3, 0.8)
    head_gain = jnp.clip(1.0 + 0.18 * jax.random.normal(splits[5], (DV,), jnp.float32), 0.1, 1.9)
    out_weight = bell_draw(splits[6], (ATTN, D), ATTN ** -0.5, 0.1875)
    mixer_gain = jnp.clip(1.0 + 0.18 * jax.random.normal(splits[7], (D,), jnp.float32), 0.1, 1.9)
    up_weight = bell_draw(splits[8], (D, FF), D ** -0.5, 0.125, ((0, 32), (1, 4)))
    down_weight = bell_draw(splits[9], (FF, D), FF ** -0.5, 0.09375, ((0, 4), (1, 32)))
    return {"tokens": tokens, "queries": queries, "keys": keys, "values": values, "lambdas": lambdas, "head_gain": head_gain, "out_weight": out_weight, "mixer_gain": mixer_gain, "up_weight": up_weight, "down_weight": down_weight}


def reference(tokens, queries, keys, values, lambdas, head_gain, out_weight, mixer_gain, up_weight, down_weight):
    query_heads = jnp.transpose(queries.astype(jnp.float32).reshape(TOKENS, HEADS, 2, DQK), (1, 2, 0, 3))
    key_heads = jnp.transpose(keys.astype(jnp.float32).reshape(TOKENS, HEADS, 2, DQK), (1, 2, 0, 3))
    value_heads = jnp.transpose(values.astype(jnp.float32).reshape(TOKENS, HEADS, DV), (1, 0, 2))
    block_rows = math.gcd(TOKENS, 512)
    positions = jnp.arange(TOKENS, dtype=jnp.int32)

    def one_head(inputs):
        query_pair, key_pair, value_rows, lam_value = inputs

        def one_block(block_index):
            offset = (block_index * block_rows).astype(jnp.int32)
            query_pos = offset + jnp.arange(block_rows, dtype=jnp.int32)
            allowed = positions[None, :] <= query_pos[:, None]
            head_maps = []
            for map_index in range(2):
                query_rows = lax.dynamic_slice_in_dim(query_pair[map_index], offset, block_rows, 0)
                scores = jnp.dot(query_rows, key_pair[map_index].T, precision=lax.Precision.HIGHEST, preferred_element_type=jnp.float32) * DQK ** (-0.5)
                scores = jnp.where(allowed, scores, -jnp.inf)
                row_max = lax.optimization_barrier(jnp.max(scores, axis=1, keepdims=True))
                exponent = jnp.exp(scores - row_max)
                row_total = lax.optimization_barrier(jnp.sum(exponent, axis=1, keepdims=True))
                weights = lax.optimization_barrier(exponent.astype(jnp.bfloat16)).astype(jnp.float32)
                head_maps.append(jnp.dot(weights, value_rows, precision=lax.Precision.HIGHEST, preferred_element_type=jnp.float32) / row_total)
            differ = head_maps[0] - lam_value * head_maps[1]
            spread = lax.rsqrt(lax.optimization_barrier(jnp.mean(differ * differ, axis=1, keepdims=True)) + 1e-06)
            return (differ * spread * head_gain).astype(jnp.bfloat16)
        return lax.map(one_block, jnp.arange(TOKENS // block_rows, dtype=jnp.int32))
    attended = lax.map(one_head, (query_heads, key_heads, value_heads, lambdas))
    attended = jnp.transpose(attended.reshape(HEADS, TOKENS, DV), (1, 0, 2)).reshape(TOKENS, HEADS * DV)
    projected = jnp.dot(attended, out_weight, preferred_element_type=jnp.float32).astype(jnp.bfloat16)
    resid = (tokens.astype(jnp.float32) + projected.astype(jnp.float32)).astype(jnp.bfloat16)
    resid_full = resid.astype(jnp.float32)
    normed = (resid_full * lax.rsqrt(lax.optimization_barrier(jnp.mean(resid_full * resid_full, axis=1, keepdims=True)) + 1e-06) * mixer_gain).astype(jnp.bfloat16)
    hidden = jnp.square(jax.nn.relu(jnp.dot(normed, up_weight, preferred_element_type=jnp.float32))).astype(jnp.bfloat16)
    return (resid_full + jnp.dot(hidden, down_weight, preferred_element_type=jnp.float32)).astype(jnp.bfloat16)
```

```python
import functools

import jax
import jax.numpy as jnp
from jax import lax
from jax.experimental import pallas as pl
from jax.experimental.pallas import tpu as pltpu
from jax.sharding import PartitionSpec as P

DQK = 64
DV = 128
BLK = 512


def attn_kernel(chip_ref, lam_ref, gain_ref, q_ref, kv_hbm, o_ref, kv_ref, s_ref, acc_ref, sems):
    chip = chip_ref[0]
    lam = lam_ref[0]
    n_a = 2 * chip + 1
    n_b = 32 - 2 * chip
    n_long = jnp.maximum(n_a, n_b)
    n_short = jnp.minimum(n_a, n_b)

    def copy_of(t):
        rows = pl.ds(pl.multiple_of(t * BLK, BLK), BLK)
        return pltpu.make_async_copy(kv_hbm.at[rows], kv_ref.at[rows], sems.at[t])

    @pl.loop(0, n_long)
    def _(t):
        copy_of(t).start()

    ones = jnp.ones((16, BLK), jnp.bfloat16)

    def run_block(b, count, waited_from):
        q1 = (q_ref[b, :, :DQK].astype(jnp.float32) * DQK ** -0.5).astype(jnp.bfloat16)
        q2 = (q_ref[b, :, DQK:].astype(jnp.float32) * DQK ** -0.5).astype(jnp.bfloat16)
        zero = jnp.zeros_like(q1)
        q_pair = (
            jnp.concatenate([q1, zero], axis=1),
            jnp.concatenate([zero, q2], axis=1),
        )

        def one_step(t, state, masked):
            @pl.when(t >= waited_from)
            def _():
                copy_of(t).wait()

            rows = pl.ds(pl.multiple_of(t * BLK, BLK), BLK)
            key = kv_ref[rows, :DV]
            val = kv_ref[rows, DV:]
            val_t = jnp.concatenate([val.T, ones], axis=0)
            out = []
            for j in range(2):
                run_max, acc = state[2 * j], state[2 * j + 1]
                scores = lax.dot_general(
                    key, q_pair[j], (((1,), (1,)), ((), ())), preferred_element_type=jnp.float32
                )
                if masked:
                    k_pos = lax.broadcasted_iota(jnp.int32, (BLK, BLK), 0)
                    q_pos = lax.broadcasted_iota(jnp.int32, (BLK, BLK), 1)
                    scores = jnp.where(k_pos <= q_pos, scores, -1e30)
                new_max = jnp.maximum(run_max, jnp.max(scores, axis=0, keepdims=True))
                shrink = jnp.exp(run_max - new_max)
                weights = jnp.exp(scores - new_max).astype(jnp.bfloat16)
                acc = acc * shrink + jnp.dot(val_t, weights, preferred_element_type=jnp.float32)
                out += [new_max, acc]
            return tuple(out)

        top = jnp.full((1, BLK), -1e30, jnp.float32)
        empty = jnp.zeros((DV + 16, BLK), jnp.float32)
        state = lax.fori_loop(
            0, count - 1, lambda t, st: one_step(t, st, False), (top, empty, top, empty)
        )
        state = one_step(count - 1, state, True)
        map_1 = state[1][:DV] / state[1][DV : DV + 1]
        map_2 = state[3][:DV] / state[3][DV : DV + 1]
        differ = map_1 - lam * map_2
        spread = lax.rsqrt(jnp.mean(differ * differ, axis=0, keepdims=True) + 1e-06)
        out = (differ * spread).T * gain_ref[...]
        o_ref[b] = out.astype(jnp.bfloat16)

    run_block(0, n_short, 0)
    run_block(1, n_long, n_short)


def attention(chip, lam, gain, q, kv):
    rows = kv.shape[0]
    smem = pl.BlockSpec(memory_space=pltpu.SMEM)
    vmem = pl.BlockSpec(memory_space=pltpu.VMEM)
    return pl.pallas_call(
        attn_kernel,
        out_shape=jax.ShapeDtypeStruct((2, BLK, DV), jnp.bfloat16),
        in_specs=[smem, smem, vmem, vmem, pl.BlockSpec(memory_space=pl.ANY)],
        out_specs=vmem,
        scratch_shapes=[
            pltpu.VMEM((rows, 2 * DV), jnp.bfloat16),
            pltpu.VMEM((BLK, BLK), jnp.float32),
            pltpu.VMEM((DV, BLK), jnp.float32),
            pltpu.SemaphoreType.DMA((rows // BLK,)),
        ],
        compiler_params=pltpu.CompilerParams(vmem_limit_bytes=48 * 1024 * 1024),
        cost_estimate=pl.CostEstimate(
            flops=24_000_000_000, bytes_accessed=16_000_000, transcendentals=17_000_000
        ),
    )(chip, lam, gain, q, kv)


def per_device(
    tokens,
    queries,
    keys,
    values,
    lambdas,
    head_gain,
    out_weight,
    mixer_gain,
    up_weight,
    down_weight,
):
    sp = lax.axis_index("sp")
    core = sp % 2
    chip = sp // 2
    count = lax.axis_size("sp")
    chips = count // 2
    first = core == 0

    def mine(a):
        return jnp.where(first, a[:, :DV], a[:, DV:])

    def other(a):
        return jnp.where(first, a[:, DV:], a[:, :DV])

    kept = jnp.concatenate([mine(keys), mine(values)], axis=1)
    sent = jnp.concatenate([other(keys), other(values)], axis=1)
    got = lax.ppermute(sent, "sp", [(s, s ^ 1) for s in range(count)])
    kv = jnp.concatenate([jnp.where(first, kept, got), jnp.where(first, got, kept)], axis=0)
    same_core = [[2 * i + c for i in range(chips)] for c in range(2)]
    kv_all = lax.all_gather(kv, "sp", axis=0, tiled=True, axis_index_groups=same_core)

    swap = []
    keep = []
    for i in range(chips):
        swap += [(2 * i, 2 * i + 1), (2 * i + 1, 2 * (chips - 1 - i))]
        keep += [(2 * i, 2 * i), (2 * i + 1, 2 * (chips - 1 - i) + 1)]
    back_swap = [(d, s) for s, d in swap]
    back_keep = [(d, s) for s, d in keep]
    q_swap = lax.ppermute(other(queries), "sp", swap)
    q_keep = lax.ppermute(mine(queries), "sp", keep)
    q_low = jnp.where(first, q_keep, q_swap)
    q_high = jnp.where(first, q_swap, q_keep)
    ordered = chip < chips // 2
    q = jnp.stack([jnp.where(ordered, q_low, q_high), jnp.where(ordered, q_high, q_low)])
    lam = jnp.where(first, lambdas[0], lambdas[1]).reshape(1)
    out = attention(chip.reshape(1), lam, head_gain.reshape(1, DV), q, kv_all)
    o_low = jnp.where(ordered, out[0], out[1])
    o_high = jnp.where(ordered, out[1], out[0])
    r_swap = lax.ppermute(jnp.where(first, o_high, o_low), "sp", back_swap)
    r_keep = lax.ppermute(jnp.where(first, o_low, o_high), "sp", back_keep)
    attended = jnp.concatenate(
        [jnp.where(first, r_keep, r_swap), jnp.where(first, r_swap, r_keep)], axis=1
    )

    tokens_all = lax.all_gather(tokens, "tp", axis=0, tiled=True)
    all_heads = lax.all_gather(attended, "tp", axis=1, tiled=True)
    projected = jnp.dot(all_heads, out_weight, preferred_element_type=jnp.float32).astype(
        jnp.bfloat16
    )
    resid = (tokens_all.astype(jnp.float32) + projected.astype(jnp.float32)).astype(jnp.bfloat16)
    resid_full = resid.astype(jnp.float32)
    normed = (
        resid_full
        * lax.rsqrt(jnp.mean(resid_full * resid_full, axis=1, keepdims=True) + 1e-06)
        * mixer_gain
    ).astype(jnp.bfloat16)
    up_full = lax.all_gather(up_weight, "sp", axis=0, tiled=True)
    down_full = lax.all_gather(down_weight, "sp", axis=1, tiled=True)
    hidden = jnp.square(
        jax.nn.relu(jnp.dot(normed, up_full, preferred_element_type=jnp.float32))
    ).astype(jnp.bfloat16)
    partial = jnp.dot(hidden, down_full, preferred_element_type=jnp.float32).astype(jnp.bfloat16)
    rows = tokens.shape[0]
    pieces = lax.all_to_all(
        partial.reshape(-1, rows, partial.shape[1]), "tp", 0, 0, tiled=True
    )
    mixed = jnp.sum(pieces.astype(jnp.float32), axis=0)
    own = lax.dynamic_slice_in_dim(resid, lax.axis_index("tp") * rows, rows, 0)
    return (own.astype(jnp.float32) + mixed).astype(jnp.bfloat16)


def solution(mesh):
    placed = (
        P(("sp", "tp"), None),
        P("sp", "tp"),
        P("sp", "tp"),
        P("sp", "tp"),
        P("tp"),
        P(),
        P(),
        P(),
        P("sp", "tp"),
        P("tp", "sp"),
    )
    return jax.shard_map(
        per_device, mesh=mesh, in_specs=placed, out_specs=P(("sp", "tp"), None), check_vma=False
    )
```

```python
import jax
import jax.numpy as jnp
from jax import lax
from jax.experimental import pallas as pl
from jax.experimental.pallas import tpu as pltpu
from jax.sharding import PartitionSpec as P

MESH = pl.DeviceIdType.MESH
DQK = 64
DV = 128
BLK = 512
HALF = 256
RING = 4
CHIPS = 16
TP = 4
D = 2048
FFT = 1024
ROWS = 128
SUMROWS = 16

HERE, LEFT, RIGHT, FAR = 0, 1, 2, 3
FIRST = (HERE, LEFT, RIGHT, HERE, HERE, FAR, HERE, LEFT, LEFT, RIGHT, RIGHT, LEFT, RIGHT, FAR, FAR, FAR)
SECOND = (HERE, HERE, HERE, LEFT, RIGHT, HERE, FAR, LEFT, RIGHT, LEFT, RIGHT, FAR, FAR, LEFT, RIGHT, FAR)


def pick(index, table):
    value = jnp.int32(0)
    for at, entry in enumerate(table):
        if entry:
            value = value + jnp.where(index == at, entry, 0)
    return value


def shift(place):
    return jnp.where(place == LEFT, 3, jnp.where(place == RIGHT, 1, jnp.where(place == FAR, 2, 0)))


def remote(src, dst, send_sem, recv_sem, sp, tp):
    return pltpu.make_async_remote_copy(
        src_ref=src,
        dst_ref=dst,
        send_sem=send_sem,
        recv_sem=recv_sem,
        device_id=(sp, tp),
        device_id_type=MESH,
    )


def layer_kernel(
    tokens,
    queries,
    keys,
    values,
    lambdas,
    head_gain,
    out_weight,
    mixer_gain,
    up_weight,
    down_weight,
    result,
    kv,
    q_in,
    q_t,
    v_t,
    run_max,
    acc,
    weights,
    out_w,
    tok,
    stage,
    att,
    resid,
    normed,
    part,
    relay,
    arrived,
    own_sem,
    load_sem,
    swap_sem,
    q_sem,
    kv_send,
    kv_recv,
    w_send,
    w_recv,
    pair_send,
    pair_recv,
    tok_send,
    tok_recv,
    back_send,
    back_recv,
    att_send,
    att_recv,
    sum_send,
    sum_recv,
):
    sp = lax.axis_index("sp")
    x = lax.axis_index("tp")
    core = lax.rem(sp, 2)
    chip = sp // 2
    y = lax.rem(chip, RING)
    z = chip // RING
    mirror = CHIPS - 1 - chip
    pair = chip * 2 + (1 - core)

    def ring(place, step):
        return lax.rem(place + step, RING)

    def at(yy, zz):
        return (zz * RING + yy) * 2 + core

    y_up, y_down = at(ring(y, 1), z), at(ring(y, 3), z)
    z_up, z_down = at(y, ring(z, 1)), at(y, ring(z, 3))
    x_up, x_down = ring(x, 1), ring(x, 3)

    barrier = pltpu.get_barrier_semaphore()
    greeted = [(s, x) for s in (y_up, y_down, z_up, z_down, pair, mirror * 2, mirror * 2 + 1)]
    greeted += [(sp, x_up), (sp, x_down)]
    for device in greeted:
        pl.semaphore_signal(barrier, inc=1, device_id=device, device_id_type=MESH)
    pl.semaphore_wait(barrier, len(greeted))

    def lanes(place):
        return pl.ds(pl.multiple_of(place * DV, DV), DV)

    mine = lanes(core)
    theirs = lanes(1 - core)
    own_q = pltpu.make_async_copy(queries.at[:, pl.ds(0, DV)], q_in.at[0], own_sem.at[0])

    def q_copy(head, slot, to):
        return remote(
            queries.at[:, pl.ds(head * DV, DV)], q_in.at[slot], q_sem.at[2 + head], q_sem.at[slot], to, x
        )

    @pl.when(core == 0)
    def _():
        q_copy(1, 0, pair).start()
        own_q.start()

    @pl.when(core == 1)
    def _():
        q_copy(0, 1, mirror * 2).start()
        q_copy(1, 1, mirror * 2 + 1).start()

    own_block = pl.ds((chip * 2 + core) * 2, 2)
    pair_block = pl.ds((chip * 2 + 1 - core) * 2, 2)
    swaps = []
    owns = []
    for number, (array, half) in enumerate(((keys, pl.ds(0, DV)), (values, pl.ds(DV, DV)))):
        for unit in range(2):
            rows = pl.ds(unit * HALF, HALF)
            place = kv.at[(chip * 2 + core) * 2 + unit, :, half]
            index = number * 2 + unit
            swaps.append(
                remote(array.at[rows, theirs], place, swap_sem.at[4 + index], swap_sem.at[index], pair, x)
            )
            owns.append(pltpu.make_async_copy(array.at[rows, mine], place, own_sem.at[1 + index]))
    for copy in swaps + owns:
        copy.start()

    own_tok = pltpu.make_async_copy(tokens, tok.at[x], own_sem.at[5])
    own_tok.start()

    def tok_copy(source, unit, to, fwd):
        rows = pl.ds(unit * (ROWS // 2), ROWS // 2)
        return remote(
            tok.at[source, rows], tok.at[source, rows], tok_send.at[fwd], tok_recv.at[source, unit], sp, to
        )

    own_w = []
    w_row = chip * 128 + core * 64
    for number, array in enumerate((up_weight, down_weight)):
        own_w.append(
            pltpu.make_async_copy(
                array, weights.at[number, pl.ds(pl.multiple_of(w_row, 64), 64)], own_sem.at[6 + number]
            )
        )
        own_w[-1].start()
    load_w = pltpu.make_async_copy(out_weight, out_w, load_sem.at[0])
    load_w.start()

    run_max[...] = jnp.full(run_max.shape, -1e30, jnp.float32)
    acc[...] = jnp.zeros(acc.shape, jnp.float32)
    v_t[DV:, :] = jnp.ones((SUMROWS, BLK), jnp.bfloat16)

    own_tok.wait()
    for unit in range(2):
        for number, to in enumerate((x_up, x_down)):
            tok_copy(x, unit, to, unit * 2 + number).start()

    for copy in owns:
        copy.wait()
    for copy in swaps:
        copy.wait_recv()

    @pl.when(core == 0)
    def _():
        own_q.wait()

    @pl.when(core == 1)
    def _():
        q_copy(0, 0, pair).wait_recv()

    q_copy(0, 1, mirror * 2).wait_recv()

    for slot in range(2):
        q_slot = (q_in[slot].astype(jnp.float32) * DQK ** -0.5).T.astype(jnp.bfloat16)
        zero = jnp.zeros((DQK, BLK), jnp.bfloat16)
        q_t[slot, 0, :DQK] = q_slot[:DQK]
        q_t[slot, 0, DQK:] = zero
        q_t[slot, 1, :DQK] = zero
        q_t[slot, 1, DQK:] = q_slot[DQK:]

    def gather_event(number, unit_ref, send_sem, recv_ref):
        odd = lax.rem(number, 2)
        first = pick(number // 2, FIRST)
        second = pick(number // 2, SECOND)
        y_step = jnp.where(odd == 0, shift(first), shift(second))
        z_step = jnp.where(odd == 0, shift(second), shift(first))
        source = ring(z, z_step) * RING + ring(y, y_step)
        first_up = jnp.where(odd == 0, y_up, z_up)
        first_down = jnp.where(odd == 0, y_down, z_down)
        second_up = jnp.where(odd == 0, z_up, y_up)
        second_down = jnp.where(odd == 0, z_down, y_down)

        def copy(unit, to):
            ref = unit_ref(odd, source, unit)
            return remote(ref, ref, send_sem, recv_ref(odd, source, unit), to, x)

        @pl.when(number >= 2)
        def _():
            for unit in range(2):
                copy(unit, sp).wait_recv()

        for unit in range(2):
            along = LEFT if unit == 0 else RIGHT
            on_first = (second == HERE) & ((first == HERE) | (first == along))
            at_start = (second == HERE) & (first == HERE)
            on_second = (second == HERE) | (second == along)
            at_turn = second == HERE
            for to, sends in (
                (first_up, on_first if unit == 0 else at_start),
                (first_down, at_start if unit == 0 else on_first),
                (second_up, on_second if unit == 0 else at_turn),
                (second_down, at_turn if unit == 0 else on_second),
            ):

                @pl.when(sends)
                def _(unit=unit, to=to):
                    copy(unit, to).start()

        return odd, source

    def kv_unit(odd, source, unit):
        return kv.at[(source * 2 + odd) * 2 + unit]

    def kv_sem(odd, source, unit):
        return kv_recv.at[(source * 2 + odd) * 2 + unit]

    def kv_body(number, carry):
        odd, source = gather_event(number, kv_unit, kv_send.at[0], kv_sem)
        block = source * 2 + odd

        @pl.when(number == 10)
        def _():
            for unit in range(2):
                tok_copy(x_down, unit, x_up, 0).wait_recv()
                tok_copy(x_up, unit, x_down, 0).wait_recv()
            tok_copy(x_down, 0, x_up, 4).start()
            tok_copy(x_up, 1, x_down, 5).start()

        key = kv[pl.ds(block * 2, 2), :, :DV].reshape(BLK, DV)
        v_t[:DV, :] = kv[pl.ds(block * 2, 2), :, DV:].reshape(BLK, DV).T

        def step(slot, masked):
            for j in range(2):
                scores = jnp.dot(key, q_t[slot, j], preferred_element_type=jnp.float32)
                if masked:
                    k_pos = lax.broadcasted_iota(jnp.int32, (BLK, BLK), 0)
                    q_pos = lax.broadcasted_iota(jnp.int32, (BLK, BLK), 1)
                    scores = jnp.where(k_pos <= q_pos, scores, -1e30)
                old_max = run_max[slot, j]
                new_max = jnp.maximum(old_max, jnp.max(scores, axis=0, keepdims=True))
                shrink = jnp.exp(old_max - new_max)
                weight = jnp.exp(scores - new_max).astype(jnp.bfloat16)
                acc[slot, j] = acc[slot, j] * shrink + jnp.dot(
                    v_t[...], weight, preferred_element_type=jnp.float32
                )
                run_max[slot, j] = new_max

        def slot_body(slot, inner):
            q_block = jnp.where(slot == 0, chip * 2, 31 - chip * 2)

            @pl.when(block < q_block)
            def _():
                step(slot, False)

            @pl.when(block == q_block)
            def _():
                step(slot, True)

            return inner

        lax.fori_loop(0, 2, slot_body, 0)
        return carry

    lax.fori_loop(0, 2 * CHIPS, kv_body, 0)

    def w_unit(odd, source, unit):
        return weights.at[odd, pl.ds(pl.multiple_of(source * 128 + core * 64 + unit * 32, 32), 32)]

    def w_sem(odd, source, unit):
        return w_recv.at[odd, source * 2 + unit]

    def w_body(number, carry):
        odd, source = gather_event(number, w_unit, w_send.at[0], w_sem)
        item = weights.at[odd, pl.ds(pl.multiple_of(source * 128 + core * 64, 64), 64)]
        remote(item, item, pair_send.at[0], pair_recv.at[0], pair, x).start()
        return carry

    for copy in own_w:
        copy.wait()
    lax.fori_loop(0, 2, w_body, 0)

    for slot in range(2):
        map_1 = acc[slot, 0, :DV] / acc[slot, 0, DV : DV + 1]
        map_2 = acc[slot, 1, :DV] / acc[slot, 1, DV : DV + 1]
        lam = jnp.where(core == 0, lambdas[0], lambdas[1])
        differ = map_1 - lam * map_2
        spread = lax.rsqrt(jnp.mean(differ * differ, axis=0, keepdims=True) + 1e-06)
        stage[slot] = ((differ * spread).T * head_gain[...]).astype(jnp.bfloat16)

    def att_lanes(head):
        return pl.ds(pl.multiple_of((x * 2 + head) * DV, DV), DV)

    def back_copy(slot, head, to):
        return remote(
            stage.at[slot], att.at[:, att_lanes(head)], back_send.at[slot], back_recv.at[head], to, x
        )

    @pl.when(core == 0)
    def _():
        att[:, att_lanes(0)] = stage[0]

    @pl.when(core == 1)
    def _():
        back_copy(0, 1, pair).start()

    back_copy(1, core, mirror * 2 + 1).start()

    lax.fori_loop(2, 10, w_body, 0)

    @pl.when(core == 1)
    def _():
        back_copy(0, 0, pair).wait_recv()

    back_copy(0, 1, pair).wait_recv()

    def att_copy(source, unit, to, sem):
        place = att.at[
            pl.ds(unit * HALF, HALF), pl.ds(pl.multiple_of(source * 2 * DV, 2 * DV), 2 * DV)
        ]
        return remote(place, place, att_send.at[sem], att_recv.at[source, unit], sp, to)

    for unit in range(2):
        for number, to in enumerate((x_up, x_down)):
            att_copy(x, unit, to, unit * 2 + number).start()

    lax.fori_loop(10, 20, w_body, 0)

    for unit in range(2):
        att_copy(x_down, unit, x_up, 0).wait_recv()
        att_copy(x_up, unit, x_down, 0).wait_recv()
    att_copy(x_down, 0, x_up, 4).start()
    att_copy(x_up, 1, x_down, 5).start()

    lax.fori_loop(20, 2 * CHIPS, w_body, 0)

    x_far = ring(x, 2)
    load_w.wait()
    for unit in range(2):
        tok_copy(x_far, unit, x_up, 0).wait_recv()
    for unit in range(2):
        att_copy(x_far, unit, x_up, 0).wait_recv()

    @pl.loop(0, 4)
    def _(column):
        cols = pl.ds(pl.multiple_of(column * 512, 512), 512)
        projected = jnp.dot(att[...], out_w[:, cols], preferred_element_type=jnp.float32).astype(
            jnp.bfloat16
        )
        tok_cols = tok[:, :, cols].reshape(BLK, 512)
        resid[:, cols] = (tok_cols.astype(jnp.float32) + projected.astype(jnp.float32)).astype(
            jnp.bfloat16
        )

    @pl.loop(0, 8)
    def _(tile):
        rows = pl.ds(pl.multiple_of(tile * 64, 64), 64)
        full = resid[rows].astype(jnp.float32)
        scale = lax.rsqrt(jnp.mean(full * full, axis=1, keepdims=True) + 1e-06)
        normed[rows] = (full * scale * mixer_gain[...]).astype(jnp.bfloat16)

    remote(weights.at[0], weights.at[0], pair_send.at[0], pair_recv.at[0], pair, x).wait_recv()

    def hidden_of(owner):
        rows = pl.ds(pl.multiple_of(owner * ROWS, ROWS), ROWS)
        hidden = jnp.dot(normed[rows], weights[0], preferred_element_type=jnp.float32)
        return jnp.square(jnp.maximum(hidden, 0.0)).astype(jnp.bfloat16)

    def down(hidden, column, width):
        return lax.dot_general(
            hidden,
            weights[1, column : column + width],
            (((1,), (1,)), ((), ())),
            preferred_element_type=jnp.float32,
        )

    wide = D // 2

    def relay_copy(number, to):
        return remote(
            part.at[0, number], relay.at[number], sum_send.at[number], sum_recv.at[number], sp, to
        )

    def final_copy(number, half, to):
        return remote(
            part.at[1 + number, half],
            arrived.at[number, half],
            sum_send.at[2 + number * 2 + half],
            sum_recv.at[2 + number * 2 + half],
            sp,
            to,
        )

    hidden = hidden_of(x_far)
    for half, to in ((0, x_up), (1, x_down)):
        part[0, half] = down(hidden, half * wide, wide).astype(jnp.bfloat16)
        relay_copy(half, to).start()

    for number, to in ((0, x_up), (1, x_down)):
        hidden = hidden_of(to)
        plain = 1 - number
        part[1 + number, plain] = down(hidden, plain * wide, wide).astype(jnp.bfloat16)
        final_copy(number, plain, to).start()
        added = down(hidden, number * wide, wide)
        relay_copy(number, to).wait_recv()
        part[1 + number, number] = (added + relay[number].astype(jnp.float32)).astype(jnp.bfloat16)
        final_copy(number, number, to).start()

    hidden = hidden_of(x)
    own_rows = pl.ds(pl.multiple_of(x * ROWS, ROWS), ROWS)
    for half in range(2):
        cols = slice(half * wide, (half + 1) * wide)
        total = down(hidden, half * wide, wide) + resid[own_rows, cols].astype(jnp.float32)
        for number in range(2):
            final_copy(number, half, x_up).wait_recv()
            total = total + arrived[number, half].astype(jnp.float32)
        result[:, cols] = total.astype(jnp.bfloat16)

    @pl.when(core == 0)
    def _():
        q_copy(1, 0, pair).wait_send()

    @pl.when(core == 1)
    def _():
        q_copy(0, 1, mirror * 2).wait_send()
        q_copy(1, 1, mirror * 2 + 1).wait_send()
        back_copy(0, 1, pair).wait_send()

    for copy in swaps:
        copy.wait_send()
    for sem in range(6):
        tok_copy(x, 0, x_up, sem).wait_send()
        att_copy(x, 0, x_up, sem).wait_send()
    sent_kv = kv.at[pl.ds(0, 60)]
    remote(sent_kv, sent_kv, kv_send.at[0], kv_recv.at[0], y_up, x).wait_send()
    sent_w = weights.at[0, pl.ds(0, 60 * 32)]
    remote(sent_w, sent_w, w_send.at[0], w_recv.at[0, 0], y_up, x).wait_send()
    remote(weights.at[0], weights.at[0], pair_send.at[0], pair_recv.at[0], pair, x).wait_send()
    back_copy(1, core, mirror * 2 + 1).wait_send()
    for number in range(2):
        relay_copy(number, x_up).wait_send()
        for half in range(2):
            final_copy(number, half, x_up).wait_send()


def per_device(
    tokens,
    queries,
    keys,
    values,
    lambdas,
    head_gain,
    out_weight,
    mixer_gain,
    up_weight,
    down_weight,
):
    any_ref = pl.BlockSpec(memory_space=pl.ANY)
    vmem = pl.BlockSpec(memory_space=pltpu.VMEM)
    smem = pl.BlockSpec(memory_space=pltpu.SMEM)
    bf16, f32 = jnp.bfloat16, jnp.float32
    dma = pltpu.SemaphoreType.DMA
    return pl.pallas_call(
        layer_kernel,
        out_shape=jax.ShapeDtypeStruct(tokens.shape, bf16),
        in_specs=[any_ref] * 4 + [smem, vmem, any_ref, vmem, any_ref, any_ref],
        out_specs=vmem,
        scratch_shapes=[
            pltpu.VMEM((64, HALF, 2 * DV), bf16),
            pltpu.VMEM((2, BLK, DV), bf16),
            pltpu.VMEM((2, 2, DV, BLK), bf16),
            pltpu.VMEM((DV + SUMROWS, BLK), bf16),
            pltpu.VMEM((2, 2, 1, BLK), f32),
            pltpu.VMEM((2, 2, DV + SUMROWS, BLK), f32),
            pltpu.VMEM((2, D, FFT), bf16),
            pltpu.VMEM((1024, D), bf16),
            pltpu.VMEM((TP, ROWS, D), bf16),
            pltpu.VMEM((2, BLK, DV), bf16),
            pltpu.VMEM((BLK, 1024), bf16),
            pltpu.VMEM((BLK, D), bf16),
            pltpu.VMEM((BLK, D), bf16),
            pltpu.VMEM((3, 2, ROWS, D // 2), bf16),
            pltpu.VMEM((2, ROWS, D // 2), bf16),
            pltpu.VMEM((2, 2, ROWS, D // 2), bf16),
            dma((8,)),
            dma((1,)),
            dma((8,)),
            dma((4,)),
            dma((1,)),
            dma((64,)),
            dma((1,)),
            dma((2, 32)),
            dma((1,)),
            dma((1,)),
            dma((6,)),
            dma((TP, 2)),
            dma((2,)),
            dma((2,)),
            dma((6,)),
            dma((TP, 2)),
            dma((6,)),
            dma((6,)),
        ],
        compiler_params=pltpu.CompilerParams(
            collective_id=0, has_side_effects=True, vmem_limit_bytes=56 * 1024 * 1024
        ),
    )(
        tokens,
        queries,
        keys,
        values,
        lambdas,
        head_gain.reshape(1, -1),
        out_weight,
        mixer_gain.reshape(1, -1),
        up_weight,
        down_weight.T,
    )


def solution(mesh):
    placed = (
        P(("sp", "tp"), None),
        P("sp", "tp"),
        P("sp", "tp"),
        P("sp", "tp"),
        P("tp"),
        P(),
        P(),
        P(),
        P("sp", "tp"),
        P("tp", "sp"),
    )
    return jax.shard_map(
        per_device, mesh=mesh, in_specs=placed, out_specs=P(("sp", "tp"), None), check_vma=False
    )
```

```python
import jax
import jax.numpy as jnp
from jax import lax
from jax.experimental import pallas as pl
from jax.experimental.pallas import tpu as pltpu
from jax.sharding import PartitionSpec as P

MESH = pl.DeviceIdType.MESH
DQK = 64
DV = 128
BLK = 512
HALF = 256
RING = 4
CHIPS = 16
TP = 4
D = 2048
FFT = 1024
ROWS = 128
SUMROWS = 16
W_FROM = 26

HERE, LEFT, RIGHT, FAR = 0, 1, 2, 3
FIRST = (HERE, LEFT, RIGHT, HERE, HERE, FAR, HERE, LEFT, LEFT, RIGHT, RIGHT, LEFT, RIGHT, FAR, FAR, FAR)
SECOND = (HERE, HERE, HERE, LEFT, RIGHT, HERE, FAR, LEFT, RIGHT, LEFT, RIGHT, FAR, FAR, LEFT, RIGHT, FAR)


def pick(index, table):
    value = jnp.int32(0)
    for at, entry in enumerate(table):
        if entry:
            value = value + jnp.where(index == at, entry, 0)
    return value


def shift(place):
    return jnp.where(place == LEFT, 3, jnp.where(place == RIGHT, 1, jnp.where(place == FAR, 2, 0)))


def remote(src, dst, send_sem, recv_sem, sp, tp):
    return pltpu.make_async_remote_copy(
        src_ref=src,
        dst_ref=dst,
        send_sem=send_sem,
        recv_sem=recv_sem,
        device_id=(sp, tp),
        device_id_type=MESH,
    )


def layer_kernel(
    tokens,
    queries,
    keys,
    values,
    lambdas,
    head_gain,
    out_weight,
    mixer_gain,
    up_weight,
    down_weight,
    result,
    kv,
    q_in,
    q_t,
    v_t,
    scores_a,
    scores_b,
    top,
    run_max,
    acc,
    weights,
    out_w,
    tok,
    stage,
    att,
    resid,
    normed,
    part,
    relay,
    arrived,
    own_sem,
    load_sem,
    swap_sem,
    q_sem,
    kv_send,
    kv_recv,
    w_send,
    w_recv,
    pair_send,
    pair_recv,
    tok_send,
    tok_recv,
    back_send,
    back_recv,
    att_send,
    att_recv,
    sum_send,
    sum_recv,
):
    sp = lax.axis_index("sp")
    x = lax.axis_index("tp")
    core = lax.rem(sp, 2)
    chip = sp // 2
    y = lax.rem(chip, RING)
    z = chip // RING
    mirror = CHIPS - 1 - chip
    pair = chip * 2 + (1 - core)

    def ring(place, step):
        return lax.rem(place + step, RING)

    def at(yy, zz):
        return (zz * RING + yy) * 2 + core

    y_up, y_down = at(ring(y, 1), z), at(ring(y, 3), z)
    z_up, z_down = at(y, ring(z, 1)), at(y, ring(z, 3))
    x_up, x_down = ring(x, 1), ring(x, 3)

    barrier = pltpu.get_barrier_semaphore()
    greeted = [(s, x) for s in (y_up, y_down, z_up, z_down, pair, mirror * 2, mirror * 2 + 1)]
    greeted += [(sp, x_up), (sp, x_down)]
    for device in greeted:
        pl.semaphore_signal(barrier, inc=1, device_id=device, device_id_type=MESH)
    pl.semaphore_wait(barrier, len(greeted))

    def lanes(place):
        return pl.ds(pl.multiple_of(place * DV, DV), DV)

    mine = lanes(core)
    theirs = lanes(1 - core)
    own_q = pltpu.make_async_copy(queries.at[:, pl.ds(0, DV)], q_in.at[0], own_sem.at[0])

    def q_copy(head, slot, to):
        return remote(
            queries.at[:, pl.ds(head * DV, DV)], q_in.at[slot], q_sem.at[2 + head], q_sem.at[slot], to, x
        )

    @pl.when(core == 0)
    def _():
        q_copy(1, 0, pair).start()
        own_q.start()

    @pl.when(core == 1)
    def _():
        q_copy(0, 1, mirror * 2).start()
        q_copy(1, 1, mirror * 2 + 1).start()

    own_block = pl.ds((chip * 2 + core) * 2, 2)
    pair_block = pl.ds((chip * 2 + 1 - core) * 2, 2)
    swaps = []
    owns = []
    for number, (array, half) in enumerate(((keys, pl.ds(0, DV)), (values, pl.ds(DV, DV)))):
        for unit in range(2):
            rows = pl.ds(unit * HALF, HALF)
            place = kv.at[(chip * 2 + core) * 2 + unit, :, half]
            index = number * 2 + unit
            swaps.append(
                remote(array.at[rows, theirs], place, swap_sem.at[4 + index], swap_sem.at[index], pair, x)
            )
            owns.append(pltpu.make_async_copy(array.at[rows, mine], place, own_sem.at[1 + index]))
    for copy in swaps + owns:
        copy.start()

    own_tok = pltpu.make_async_copy(tokens, tok.at[x], own_sem.at[5])
    own_tok.start()

    def tok_copy(source, unit, to, fwd):
        rows = pl.ds(unit * (ROWS // 2), ROWS // 2)
        return remote(
            tok.at[source, rows], tok.at[source, rows], tok_send.at[fwd], tok_recv.at[source, unit], sp, to
        )

    own_w = []
    w_row = chip * 128 + core * 64
    for number, array in enumerate((up_weight, down_weight)):
        own_w.append(
            pltpu.make_async_copy(
                array, weights.at[number, pl.ds(pl.multiple_of(w_row, 64), 64)], own_sem.at[6 + number]
            )
        )
        own_w[-1].start()
    load_w = pltpu.make_async_copy(out_weight, out_w, load_sem.at[0])
    load_w.start()

    run_max[...] = jnp.full(run_max.shape, -1e30, jnp.float32)
    acc[...] = jnp.zeros(acc.shape, jnp.float32)
    v_t[...] = jnp.ones(v_t.shape, jnp.bfloat16)
    scores_b[...] = jnp.full(scores_b.shape, -1e30, jnp.float32)
    top[...] = jnp.full(top.shape, -1e30, jnp.float32)

    own_tok.wait()
    for unit in range(2):
        for number, to in enumerate((x_up, x_down)):
            tok_copy(x, unit, to, unit * 2 + number).start()

    for copy in owns:
        copy.wait()
    for copy in swaps:
        copy.wait_recv()

    def item_of(number):
        odd = lax.rem(number, 2)
        first = pick(number // 2, FIRST)
        second = pick(number // 2, SECOND)
        y_step = jnp.where(odd == 0, shift(first), shift(second))
        z_step = jnp.where(odd == 0, shift(second), shift(first))
        source = ring(z, z_step) * RING + ring(y, y_step)
        return odd, first, second, source

    def pass_on(number, ref_of, send_sem, recv_of):
        odd, first, second, source = item_of(number)
        first_up = jnp.where(odd == 0, y_up, z_up)
        first_down = jnp.where(odd == 0, y_down, z_down)
        second_up = jnp.where(odd == 0, z_up, y_up)
        second_down = jnp.where(odd == 0, z_down, y_down)
        at_turn = second == HERE
        at_start = at_turn & (first == HERE)
        halves = (second == FAR) | (at_turn & (first == FAR))

        def copy(unit, to):
            ref = ref_of(odd, source, unit)
            return remote(ref, ref, send_sem, recv_of(odd, source, 0 if unit is None else unit), to, x)

        @pl.when(jnp.logical_not(at_start) & halves)
        def _():
            copy(0, sp).wait_recv()
            copy(1, sp).wait_recv()

        @pl.when(jnp.logical_not(at_start | halves))
        def _():
            copy(None, sp).wait_recv()

        for unit, to, sends in (
            (None, first_up, at_start),
            (None, first_down, at_start),
            (0, first_up, at_turn & (first == LEFT)),
            (1, first_down, at_turn & (first == RIGHT)),
            (None, second_up, at_turn),
            (None, second_down, at_turn),
            (0, second_up, second == LEFT),
            (1, second_down, second == RIGHT),
        ):

            @pl.when(sends)
            def _(unit=unit, to=to):
                copy(unit, to).start()

    def kv_ref(odd, source, unit):
        first = (source * 2 + odd) * 2
        return kv.at[pl.ds(first, 2)] if unit is None else kv.at[first + unit]

    def kv_sem(odd, source, unit):
        return kv_recv.at[(source * 2 + odd) * 2 + unit]

    def kv_pass(number, carry):
        pass_on(number, kv_ref, kv_send.at[0], kv_sem)
        return carry

    lax.fori_loop(0, 2, kv_pass, 0)

    @pl.when(core == 0)
    def _():
        own_q.wait()

    @pl.when(core == 1)
    def _():
        q_copy(0, 0, pair).wait_recv()

    q_copy(0, 1, mirror * 2).wait_recv()

    for slot in range(2):
        q_slot = (q_in[slot].astype(jnp.float32) * DQK ** -0.5).T.astype(jnp.bfloat16)
        zero = jnp.zeros((DQK, BLK), jnp.bfloat16)
        q_t[slot, 0, :DQK] = q_slot[:DQK]
        q_t[slot, 0, DQK:] = zero
        q_t[slot, 1, :DQK] = zero
        q_t[slot, 1, DQK:] = q_slot[DQK:]

    def w_ref(odd, source, unit):
        row = source * 128 + core * 64
        if unit is None:
            return weights.at[odd, pl.ds(pl.multiple_of(row, 64), 64)]
        return weights.at[odd, pl.ds(pl.multiple_of(row + unit * 32, 32), 32)]

    def w_sem(odd, source, unit):
        return w_recv.at[odd, source * 2 + unit]

    def w_pass(number, carry):
        pass_on(number, w_ref, w_send.at[0], w_sem)
        odd, _, _, source = item_of(number)
        item = w_ref(odd, source, None)
        remote(item, item, pair_send.at[0], pair_recv.at[0], pair, x).start()
        return carry

    scores_of = (scores_a, scores_b)

    def absorb(before, j, weight, new_max, slot):
        shrink = jnp.exp(run_max[slot, j] - new_max)
        acc[slot, j] = acc[slot, j] * shrink + jnp.dot(
            v_t[before], weight, preferred_element_type=jnp.float32
        )
        run_max[slot, j] = new_max

    def softmax(before, j, slot):
        new_max = jnp.maximum(run_max[slot, j], top[before, j])
        weight = jnp.exp(scores_of[before][j] - new_max).astype(jnp.bfloat16)
        return weight, new_max

    def step(now, block, slot, last_slot, masked):
        before = 1 - now
        key = kv[pl.ds(block * 2, 2), :, :DV].reshape(BLK, DV)
        v_t[now, :DV, :] = kv[pl.ds(block * 2, 2), :, DV:].reshape(BLK, DV).T
        for j in range(2):
            scores = jnp.dot(key, q_t[slot, j], preferred_element_type=jnp.float32)
            if masked:
                k_pos = lax.broadcasted_iota(jnp.int32, (BLK, BLK), 0)
                q_pos = lax.broadcasted_iota(jnp.int32, (BLK, BLK), 1)
                scores = jnp.where(k_pos <= q_pos, scores, -1e30)
            scores_of[now][j] = scores
            top[now, j] = jnp.max(scores, axis=0, keepdims=True)
            weight, new_max = softmax(before, j, last_slot)
            absorb(before, j, weight, new_max, last_slot)

    def kv_body(number, carry):
        @pl.when(number >= 2)
        def _():
            kv_pass(number, 0)

        @pl.when(number >= W_FROM)
        def _():
            w_pass(number - W_FROM, 0)

        @pl.when(number == 10)
        def _():
            for unit in range(2):
                tok_copy(x_down, unit, x_up, 0).wait_recv()
                tok_copy(x_up, unit, x_down, 0).wait_recv()
            tok_copy(x_down, 0, x_up, 4).start()
            tok_copy(x_up, 1, x_down, 5).start()

        odd, _, _, source = item_of(number)
        block = source * 2 + odd

        def slot_body(slot, inner):
            now, last_slot = inner
            q_block = jnp.where(slot == 0, chip * 2, 31 - chip * 2)
            for parity in range(2):
                for masked in (False, True):
                    wanted = (block == q_block) if masked else (block < q_block)

                    @pl.when((now == parity) & wanted)
                    def _(parity=parity, masked=masked):
                        step(parity, block, slot, last_slot, masked)

            done = block <= q_block
            return jnp.where(done, 1 - now, now), jnp.where(done, slot, last_slot)

        return lax.fori_loop(0, 2, slot_body, carry)

    for copy in own_w:
        copy.wait()
    _, last_slot = lax.fori_loop(0, 2 * CHIPS, kv_body, (jnp.int32(0), jnp.int32(0)))
    for j in range(2):
        weight, new_max = softmax(0, j, last_slot)
        absorb(0, j, weight, new_max, last_slot)

    for slot in range(2):
        map_1 = acc[slot, 0, :DV] / acc[slot, 0, DV : DV + 1]
        map_2 = acc[slot, 1, :DV] / acc[slot, 1, DV : DV + 1]
        lam = jnp.where(core == 0, lambdas[0], lambdas[1])
        differ = map_1 - lam * map_2
        spread = lax.rsqrt(jnp.mean(differ * differ, axis=0, keepdims=True) + 1e-06)
        stage[slot] = ((differ * spread).T * head_gain[...]).astype(jnp.bfloat16)

    def att_lanes(head):
        return pl.ds(pl.multiple_of((x * 2 + head) * DV, DV), DV)

    def back_copy(slot, head, to):
        return remote(
            stage.at[slot], att.at[:, att_lanes(head)], back_send.at[slot], back_recv.at[head], to, x
        )

    @pl.when(core == 0)
    def _():
        att[:, att_lanes(0)] = stage[0]

    @pl.when(core == 1)
    def _():
        back_copy(0, 1, pair).start()

    back_copy(1, core, mirror * 2 + 1).start()

    lax.fori_loop(2 * CHIPS - W_FROM, 12, w_pass, 0)

    @pl.when(core == 1)
    def _():
        back_copy(0, 0, pair).wait_recv()

    back_copy(0, 1, pair).wait_recv()

    def att_copy(source, unit, to, sem):
        place = att.at[
            pl.ds(unit * HALF, HALF), pl.ds(pl.multiple_of(source * 2 * DV, 2 * DV), 2 * DV)
        ]
        return remote(place, place, att_send.at[sem], att_recv.at[source, unit], sp, to)

    for unit in range(2):
        for number, to in enumerate((x_up, x_down)):
            att_copy(x, unit, to, unit * 2 + number).start()

    lax.fori_loop(12, 20, w_pass, 0)

    for unit in range(2):
        att_copy(x_down, unit, x_up, 0).wait_recv()
        att_copy(x_up, unit, x_down, 0).wait_recv()
    att_copy(x_down, 0, x_up, 4).start()
    att_copy(x_up, 1, x_down, 5).start()

    lax.fori_loop(20, 30, w_pass, 0)

    x_far = ring(x, 2)
    load_w.wait()
    for unit in range(2):
        tok_copy(x_far, unit, x_up, 0).wait_recv()
    for unit in range(2):
        att_copy(x_far, unit, x_up, 0).wait_recv()

    @pl.loop(0, 4)
    def _(column):
        cols = pl.ds(pl.multiple_of(column * 512, 512), 512)
        projected = jnp.dot(att[...], out_w[:, cols], preferred_element_type=jnp.float32).astype(
            jnp.bfloat16
        )
        tok_cols = tok[:, :, cols].reshape(BLK, 512)
        resid[:, cols] = (tok_cols.astype(jnp.float32) + projected.astype(jnp.float32)).astype(
            jnp.bfloat16
        )

    @pl.loop(0, 8)
    def _(tile):
        rows = pl.ds(pl.multiple_of(tile * 64, 64), 64)
        full = resid[rows].astype(jnp.float32)
        scale = lax.rsqrt(jnp.mean(full * full, axis=1, keepdims=True) + 1e-06)
        normed[rows] = (full * scale * mixer_gain[...]).astype(jnp.bfloat16)

    lax.fori_loop(30, 2 * CHIPS, w_pass, 0)

    remote(weights.at[0], weights.at[0], pair_send.at[0], pair_recv.at[0], pair, x).wait_recv()

    def hidden_of(owner):
        rows = pl.ds(pl.multiple_of(owner * ROWS, ROWS), ROWS)
        hidden = jnp.dot(normed[rows], weights[0], preferred_element_type=jnp.float32)
        return jnp.square(jnp.maximum(hidden, 0.0)).astype(jnp.bfloat16)

    def down(hidden, column, width):
        return lax.dot_general(
            hidden,
            weights[1, column : column + width],
            (((1,), (1,)), ((), ())),
            preferred_element_type=jnp.float32,
        )

    wide = D // 2

    def relay_copy(number, to):
        return remote(
            part.at[0, number], relay.at[number], sum_send.at[number], sum_recv.at[number], sp, to
        )

    def final_copy(number, half, to):
        return remote(
            part.at[1 + number, half],
            arrived.at[number, half],
            sum_send.at[2 + number * 2 + half],
            sum_recv.at[2 + number * 2 + half],
            sp,
            to,
        )

    hidden = hidden_of(x_far)
    for half, to in ((0, x_up), (1, x_down)):
        part[0, half] = down(hidden, half * wide, wide).astype(jnp.bfloat16)
        relay_copy(half, to).start()

    for number, to in ((0, x_up), (1, x_down)):
        hidden = hidden_of(to)
        plain = 1 - number
        part[1 + number, plain] = down(hidden, plain * wide, wide).astype(jnp.bfloat16)
        final_copy(number, plain, to).start()
        added = down(hidden, number * wide, wide)
        relay_copy(number, to).wait_recv()
        part[1 + number, number] = (added + relay[number].astype(jnp.float32)).astype(jnp.bfloat16)
        final_copy(number, number, to).start()

    hidden = hidden_of(x)
    own_rows = pl.ds(pl.multiple_of(x * ROWS, ROWS), ROWS)
    for half in range(2):
        cols = slice(half * wide, (half + 1) * wide)
        total = down(hidden, half * wide, wide) + resid[own_rows, cols].astype(jnp.float32)
        for number in range(2):
            final_copy(number, half, x_up).wait_recv()
            total = total + arrived[number, half].astype(jnp.float32)
        result[:, cols] = total.astype(jnp.bfloat16)

    @pl.when(core == 0)
    def _():
        q_copy(1, 0, pair).wait_send()

    @pl.when(core == 1)
    def _():
        q_copy(0, 1, mirror * 2).wait_send()
        q_copy(1, 1, mirror * 2 + 1).wait_send()
        back_copy(0, 1, pair).wait_send()

    for copy in swaps:
        copy.wait_send()
    for sem in range(6):
        tok_copy(x, 0, x_up, sem).wait_send()
        att_copy(x, 0, x_up, sem).wait_send()
    sent_kv = kv.at[pl.ds(0, 60)]
    remote(sent_kv, sent_kv, kv_send.at[0], kv_recv.at[0], y_up, x).wait_send()
    sent_w = weights.at[0, pl.ds(0, 60 * 32)]
    remote(sent_w, sent_w, w_send.at[0], w_recv.at[0, 0], y_up, x).wait_send()
    remote(weights.at[0], weights.at[0], pair_send.at[0], pair_recv.at[0], pair, x).wait_send()
    back_copy(1, core, mirror * 2 + 1).wait_send()
    for number in range(2):
        relay_copy(number, x_up).wait_send()
        for half in range(2):
            final_copy(number, half, x_up).wait_send()


def per_device(
    tokens,
    queries,
    keys,
    values,
    lambdas,
    head_gain,
    out_weight,
    mixer_gain,
    up_weight,
    down_weight,
):
    any_ref = pl.BlockSpec(memory_space=pl.ANY)
    vmem = pl.BlockSpec(memory_space=pltpu.VMEM)
    smem = pl.BlockSpec(memory_space=pltpu.SMEM)
    bf16, f32 = jnp.bfloat16, jnp.float32
    dma = pltpu.SemaphoreType.DMA
    return pl.pallas_call(
        layer_kernel,
        out_shape=jax.ShapeDtypeStruct(tokens.shape, bf16),
        in_specs=[any_ref] * 4 + [smem, vmem, any_ref, vmem, any_ref, any_ref],
        out_specs=vmem,
        scratch_shapes=[
            pltpu.VMEM((64, HALF, 2 * DV), bf16),
            pltpu.VMEM((2, BLK, DV), bf16),
            pltpu.VMEM((2, 2, DV, BLK), bf16),
            pltpu.VMEM((2, DV + SUMROWS, BLK), bf16),
            pltpu.VMEM((2, BLK, BLK), f32),
            pltpu.VMEM((2, BLK, BLK), f32),
            pltpu.VMEM((2, 2, 1, BLK), f32),
            pltpu.VMEM((2, 2, 1, BLK), f32),
            pltpu.VMEM((2, 2, DV + SUMROWS, BLK), f32),
            pltpu.VMEM((2, D, FFT), bf16),
            pltpu.VMEM((1024, D), bf16),
            pltpu.VMEM((TP, ROWS, D), bf16),
            pltpu.VMEM((2, BLK, DV), bf16),
            pltpu.VMEM((BLK, 1024), bf16),
            pltpu.VMEM((BLK, D), bf16),
            pltpu.VMEM((BLK, D), bf16),
            pltpu.VMEM((3, 2, ROWS, D // 2), bf16),
            pltpu.VMEM((2, ROWS, D // 2), bf16),
            pltpu.VMEM((2, 2, ROWS, D // 2), bf16),
            dma((8,)),
            dma((1,)),
            dma((8,)),
            dma((4,)),
            dma((1,)),
            dma((64,)),
            dma((1,)),
            dma((2, 32)),
            dma((1,)),
            dma((1,)),
            dma((6,)),
            dma((TP, 2)),
            dma((2,)),
            dma((2,)),
            dma((6,)),
            dma((TP, 2)),
            dma((6,)),
            dma((6,)),
        ],
        compiler_params=pltpu.CompilerParams(
            collective_id=0, has_side_effects=True, vmem_limit_bytes=56 * 1024 * 1024
        ),
    )(
        tokens,
        queries,
        keys,
        values,
        lambdas,
        head_gain.reshape(1, -1),
        out_weight,
        mixer_gain.reshape(1, -1),
        up_weight,
        down_weight.T,
    )


def solution(mesh):
    placed = (
        P(("sp", "tp"), None),
        P("sp", "tp"),
        P("sp", "tp"),
        P("sp", "tp"),
        P("tp"),
        P(),
        P(),
        P(),
        P("sp", "tp"),
        P("tp", "sp"),
    )
    return jax.shard_map(
        per_device, mesh=mesh, in_specs=placed, out_specs=P(("sp", "tp"), None), check_vma=False
    )
```

```python
import jax
import jax.numpy as jnp
from jax import lax
from jax.experimental import pallas as pl
from jax.experimental.pallas import tpu as pltpu
from jax.sharding import PartitionSpec as P

MESH = pl.DeviceIdType.MESH
DQK = 64
DV = 128
BLK = 512
HALF = 256
RING = 4
CHIPS = 16
TP = 4
D = 2048
FFT = 1024
ROWS = 128
SUMROWS = 16
W_NEXT = 22
W_A, W_B, W_C = 34 - W_NEXT, 16, 20

HERE, LEFT, RIGHT, FAR = 0, 1, 2, 3
FIRST = (HERE, LEFT, RIGHT, HERE, HERE, FAR, HERE, LEFT, LEFT, RIGHT, RIGHT, LEFT, RIGHT, FAR, FAR, FAR)
SECOND = (HERE, HERE, HERE, LEFT, RIGHT, HERE, FAR, LEFT, RIGHT, LEFT, RIGHT, FAR, FAR, LEFT, RIGHT, FAR)

OWN, SWAPPED = 0, 1
KV_KIND = (OWN, SWAPPED, OWN, OWN, OWN, SWAPPED, SWAPPED, SWAPPED, OWN, OWN, SWAPPED, OWN, SWAPPED, SWAPPED, OWN, SWAPPED)
KV_PLACE = (HERE, HERE, HERE, LEFT, RIGHT, HERE, LEFT, RIGHT, LEFT, RIGHT, FAR, FAR, LEFT, RIGHT, FAR, FAR)
KV_MATE = (0, 0, 1, 0, 0, 1, 0, 0, 1, 1, 0, 0, 1, 1, 1, 1)


def pick(index, table):
    value = jnp.int32(0)
    for at, entry in enumerate(table):
        if entry:
            value = value + jnp.where(index == at, entry, 0)
    return value


def shift(place):
    return jnp.where(place == LEFT, 3, jnp.where(place == RIGHT, 1, jnp.where(place == FAR, 2, 0)))


def remote(src, dst, send_sem, recv_sem, sp, tp):
    return pltpu.make_async_remote_copy(
        src_ref=src,
        dst_ref=dst,
        send_sem=send_sem,
        recv_sem=recv_sem,
        device_id=(sp, tp),
        device_id_type=MESH,
    )


def layer_kernel(
    tokens,
    queries,
    keys,
    values,
    lambdas,
    head_gain,
    out_weight,
    mixer_gain,
    up_weight,
    down_weight,
    result,
    kv,
    q_in,
    q_given,
    kv_given,
    q_t,
    v_t,
    scores_a,
    scores_b,
    top,
    run_max,
    acc,
    weights,
    out_w,
    tok,
    stage,
    att,
    resid,
    normed,
    part,
    relay,
    arrived,
    own_sem,
    load_sem,
    swap_sem,
    q_sem,
    kv_send,
    kv_pair,
    kv_recv,
    w_send,
    w_recv,
    pair_send,
    pair_recv,
    tok_send,
    tok_recv,
    back_sem,
    att_send,
    att_recv,
    sum_send,
    sum_recv,
):
    sp = lax.axis_index("sp")
    x = lax.axis_index("tp")
    core = lax.rem(sp, 2)
    chip = sp // 2
    y = lax.rem(chip, RING)
    z = chip // RING
    mirror = 2 * CHIPS - 1 - sp
    pair = chip * 2 + (1 - core)
    side = z // 2
    mate_z = z + 1 - 2 * lax.rem(z, 2)

    def ring(place, step):
        return lax.rem(place + step, RING)

    def at(yy, zz):
        return (zz * RING + yy) * 2 + core

    y_up, y_down = at(ring(y, 1), z), at(ring(y, 3), z)
    z_up, z_down = at(y, ring(z, 1)), at(y, ring(z, 3))
    x_up, x_down = ring(x, 1), ring(x, 3)

    mate, partner = at(y, mate_z), at(y, 3 - z)

    barrier = pltpu.get_barrier_semaphore()
    greeted = [(s, x) for s in (y_up, y_down, z_up, z_down, pair, mirror)]
    greeted += [(sp, x_up), (sp, x_down)]
    for device in greeted:
        pl.semaphore_signal(barrier, inc=1, device_id=device, device_id_type=MESH)

    def lanes(place):
        return pl.ds(pl.multiple_of(place * DV, DV), DV)

    kept, given = lanes(side), lanes(1 - side)
    own_q = pltpu.make_async_copy(queries.at[:, kept], q_in.at[0], own_sem.at[0])
    load_q = pltpu.make_async_copy(queries.at[:, given], q_given, own_sem.at[8])
    swap_q = remote(q_given, q_in.at[1], q_sem.at[0], q_sem.at[1], mirror, x)
    swaps = []
    owns = []
    loads = [load_q]
    for number, (array, half) in enumerate(((keys, pl.ds(0, DV)), (values, pl.ds(DV, DV)))):
        for unit in range(2):
            rows = pl.ds(unit * HALF, HALF)
            place = kv.at[sp * 2 + unit, :, half]
            index = number * 2 + unit
            held = kv_given.at[unit, :, half]
            loads.append(pltpu.make_async_copy(array.at[rows, given], held, own_sem.at[9 + index]))
            swaps.append(
                remote(held, place, swap_sem.at[4 + index], swap_sem.at[index], partner, x)
            )
            owns.append(pltpu.make_async_copy(array.at[rows, kept], place, own_sem.at[1 + index]))
    own_tok = pltpu.make_async_copy(tokens, tok.at[x], own_sem.at[5])
    for copy in loads + owns + [own_q, own_tok]:
        copy.start()

    run_max[...] = jnp.full(run_max.shape, -1e30, jnp.float32)
    acc[...] = jnp.zeros(acc.shape, jnp.float32)
    v_t[...] = jnp.ones(v_t.shape, jnp.bfloat16)
    scores_b[...] = jnp.full(scores_b.shape, -1e30, jnp.float32)
    top[...] = jnp.full(top.shape, -1e30, jnp.float32)

    pl.semaphore_wait(barrier, len(greeted))

    for copy in loads:
        copy.wait()
    for copy in swaps:
        copy.start()
    swap_q.start()

    def tok_copy(source, unit, to, fwd):
        rows = pl.ds(unit * (ROWS // 2), ROWS // 2)
        return remote(
            tok.at[source, rows], tok.at[source, rows], tok_send.at[fwd], tok_recv.at[source, unit], sp, to
        )

    own_w = []
    w_row = chip * 128 + core * 64
    for number, array in enumerate((up_weight, down_weight)):
        own_w.append(
            pltpu.make_async_copy(
                array, weights.at[number, pl.ds(pl.multiple_of(w_row, 64), 64)], own_sem.at[6 + number]
            )
        )
        own_w[-1].start()
    load_w = pltpu.make_async_copy(out_weight, out_w, load_sem.at[0])
    load_w.start()

    for copy in owns:
        copy.wait()

    def item_of(number):
        odd = lax.rem(number, 2)
        first = pick(number // 2, FIRST)
        second = pick(number // 2, SECOND)
        y_step = jnp.where(odd == 0, shift(first), shift(second))
        z_step = jnp.where(odd == 0, shift(second), shift(first))
        source = ring(z, z_step) * RING + ring(y, y_step)
        return odd, first, second, source

    def pass_on(number, ref_of, send_sem, recv_of):
        odd, first, second, source = item_of(number)
        first_up = jnp.where(odd == 0, y_up, z_up)
        first_down = jnp.where(odd == 0, y_down, z_down)
        second_up = jnp.where(odd == 0, z_up, y_up)
        second_down = jnp.where(odd == 0, z_down, y_down)
        at_turn = second == HERE
        at_start = at_turn & (first == HERE)
        halves = (second == FAR) | (at_turn & (first == FAR))

        def copy(unit, to):
            ref = ref_of(odd, source, unit)
            return remote(ref, ref, send_sem, recv_of(odd, source, 0 if unit is None else unit), to, x)

        @pl.when(jnp.logical_not(at_start) & halves)
        def _():
            copy(0, sp).wait_recv()
            copy(1, sp).wait_recv()

        @pl.when(jnp.logical_not(at_start | halves))
        def _():
            copy(None, sp).wait_recv()

        for unit, to, sends in (
            (None, first_up, at_start),
            (None, first_down, at_start),
            (0, first_up, at_turn & (first == LEFT)),
            (1, first_down, at_turn & (first == RIGHT)),
            (None, second_up, at_turn),
            (None, second_down, at_turn),
            (0, second_up, second == LEFT),
            (1, second_down, second == RIGHT),
        ):

            @pl.when(sends)
            def _(unit=unit, to=to):
                copy(unit, to).start()

    def kv_item(number):
        kind = pick(number, KV_KIND)
        by_mate = pick(number, KV_MATE)
        place = pick(number, KV_PLACE)
        through = jnp.where(by_mate == 1, mate_z, z)
        source_z = jnp.where(kind == OWN, through, 3 - through)
        return kind, place, by_mate, source_z * RING + ring(y, shift(place))

    def kv_pass(number, carry):
        kind, place, by_mate, source = kv_item(number)
        block = source * 2 + core

        def copy(unit, to, send_sem=kv_send.at[0]):
            ref = kv.at[pl.ds(block * 2, 2)] if unit is None else kv.at[block * 2 + unit]
            recv_sem = kv_recv.at[block * 2 + (0 if unit is None else unit)]
            return remote(ref, ref, send_sem, recv_sem, to, x)

        direct = (kind == OWN) | (by_mate == 0)
        swapped_in = (kind == SWAPPED) & (place == HERE) & (by_mate == 0)
        halves = direct & (place == FAR)

        @pl.when(swapped_in)
        def _():
            for copied in swaps:
                copied.wait_recv()

        @pl.when(halves)
        def _():
            copy(0, sp).wait_recv()
            copy(1, sp).wait_recv()

        @pl.when(jnp.logical_not(swapped_in | halves | (number == 0)))
        def _():
            copy(None, sp).wait_recv()

        to_mate = (by_mate == 0) & ((kind == SWAPPED) | (place == HERE))
        for unit, to, sends in (
            (None, y_up, direct & (place == HERE)),
            (None, y_down, direct & (place == HERE)),
            (0, y_up, direct & (place == LEFT)),
            (1, y_down, direct & (place == RIGHT)),
            (None, mate, to_mate),
        ):

            @pl.when(sends)
            def _(unit=unit, to=to):
                copy(unit, to).start()

        copy(None, pair, kv_pair.at[0]).start()
        return carry

    def w_ref(odd, source, unit):
        row = source * 128 + core * 64
        if unit is None:
            return weights.at[odd, pl.ds(pl.multiple_of(row, 64), 64)]
        return weights.at[odd, pl.ds(pl.multiple_of(row + unit * 32, 32), 32)]

    def w_sem(odd, source, unit):
        return w_recv.at[odd, source * 2 + unit]

    def w_own(odd, to):
        item = w_ref(odd, chip, None)
        remote(item, item, w_send.at[0], w_sem(odd, chip, 0), to, x).start()

    def w_pass(number, carry):
        pass_on(number, w_ref, w_send.at[0], w_sem)
        odd, _, _, source = item_of(number)
        item = w_ref(odd, source, None)
        remote(item, item, pair_send.at[0], pair_recv.at[0], pair, x).start()
        return carry

    kv_pass(jnp.int32(0), 0)
    for copy in own_w:
        copy.wait()
    for odd in range(2):
        for to in (y_up, y_down, mate):
            w_own(odd, to)
        item = w_ref(odd, chip, None)
        remote(item, item, pair_send.at[0], pair_recv.at[0], pair, x).start()
    own_tok.wait()
    for unit in range(2):
        for number, to in enumerate((x_up, x_down)):
            tok_copy(x, unit, to, unit * 2 + number).start()
    kv_pass(jnp.int32(1), 0)
    for odd in range(2):
        w_own(odd, partner)
    kv_pass(jnp.int32(2), 0)
    own_q.wait()
    swap_q.wait_recv()

    for slot in range(2):
        q_slot = (q_in[slot].astype(jnp.float32) * DQK ** -0.5).T.astype(jnp.bfloat16)
        zero = jnp.zeros((DQK, BLK), jnp.bfloat16)
        q_t[slot, 0, :DQK] = q_slot[:DQK]
        q_t[slot, 0, DQK:] = zero
        q_t[slot, 1, :DQK] = zero
        q_t[slot, 1, DQK:] = q_slot[DQK:]

    scores_of = (scores_a, scores_b)

    def absorb(before, j, weight, new_max, slot):
        shrink = jnp.exp(run_max[slot, j] - new_max)
        acc[slot, j] = acc[slot, j] * shrink + jnp.dot(
            v_t[before], weight, preferred_element_type=jnp.float32
        )
        run_max[slot, j] = new_max

    def softmax(before, j, slot):
        new_max = jnp.maximum(run_max[slot, j], top[before, j])
        weight = jnp.exp(scores_of[before][j] - new_max).astype(jnp.bfloat16)
        return weight, new_max

    def step(now, block, slot, last_slot, masked):
        before = 1 - now
        key = kv[pl.ds(block * 2, 2), :, :DV].reshape(BLK, DV)
        v_t[now, :DV, :] = kv[pl.ds(block * 2, 2), :, DV:].reshape(BLK, DV).T
        for j in range(2):
            scores = jnp.dot(key, q_t[slot, j], preferred_element_type=jnp.float32)
            if masked:
                k_pos = lax.broadcasted_iota(jnp.int32, (BLK, BLK), 0)
                q_pos = lax.broadcasted_iota(jnp.int32, (BLK, BLK), 1)
                scores = jnp.where(k_pos <= q_pos, scores, -1e30)
            scores_of[now][j] = scores
            top[now, j] = jnp.max(scores, axis=0, keepdims=True)
            weight, new_max = softmax(before, j, last_slot)
            absorb(before, j, weight, new_max, last_slot)

    def kv_body(number, carry):
        item = number // 2
        passed = lax.rem(number, 2)
        _, _, _, source = kv_item(item)
        block = source * 2 + jnp.where(passed == 1, 1 - core, core)

        @pl.when((passed == 0) & (item >= 3))
        def _():
            kv_pass(item, 0)

        @pl.when(passed == 1)
        def _():
            ref = kv.at[pl.ds(block * 2, 2)]
            remote(ref, ref, kv_send.at[0], kv_recv.at[block * 2], pair, x).wait_recv()

        @pl.when(number >= W_NEXT)
        def _():
            w_pass(number - W_NEXT + 2, 0)

        @pl.when(number == 10)
        def _():
            for unit in range(2):
                tok_copy(x_down, unit, x_up, 0).wait_recv()
                tok_copy(x_up, unit, x_down, 0).wait_recv()
            tok_copy(x_down, 0, x_up, 4).start()
            tok_copy(x_up, 1, x_down, 5).start()

        def slot_body(slot, inner):
            now, last_slot = inner
            q_block = jnp.where(slot == 0, sp, mirror)
            for parity in range(2):
                for masked in (False, True):
                    wanted = (block == q_block) if masked else (block < q_block)

                    @pl.when((now == parity) & wanted)
                    def _(parity=parity, masked=masked):
                        step(parity, block, slot, last_slot, masked)

            done = block <= q_block
            return jnp.where(done, 1 - now, now), jnp.where(done, slot, last_slot)

        return lax.fori_loop(0, 2, slot_body, carry)

    _, last_slot = lax.fori_loop(0, 2 * CHIPS, kv_body, (jnp.int32(0), jnp.int32(0)))
    for j in range(2):
        weight, new_max = softmax(0, j, last_slot)
        absorb(0, j, weight, new_max, last_slot)

    def att_lanes(source, part):
        head = side if part == 0 else 1 - side
        return pl.ds(pl.multiple_of((source * 2 + head) * DV, DV), DV)

    back = remote(
        stage, att.at[:, att_lanes(x, 0)], back_sem.at[0], back_sem.at[1], mirror, x
    )

    for slot in (1, 0):
        map_1 = acc[slot, 0, :DV] / acc[slot, 0, DV : DV + 1]
        map_2 = acc[slot, 1, :DV] / acc[slot, 1, DV : DV + 1]
        lam = jnp.where(side == 0, lambdas[0], lambdas[1])
        differ = map_1 - lam * map_2
        spread = lax.rsqrt(jnp.mean(differ * differ, axis=0, keepdims=True) + 1e-06)
        attended = ((differ * spread).T * head_gain[...]).astype(jnp.bfloat16)
        if slot == 1:
            stage[...] = attended
            back.start()
        else:
            att[:, att_lanes(x, 0)] = attended

    def att_copy(source, part, unit, to, sem):
        place = att.at[pl.ds(unit * HALF, HALF), att_lanes(source, part)]
        return remote(
            place, place, att_send.at[part * 6 + sem], att_recv.at[source, part * 2 + unit], sp, to
        )

    def att_begin(part):
        for unit in range(2):
            for number, to in enumerate((x_up, x_down)):
                att_copy(x, part, unit, to, unit * 2 + number).start()

    def att_forward(part):
        for unit in range(2):
            att_copy(x_down, part, unit, x_up, 0).wait_recv()
            att_copy(x_up, part, unit, x_down, 0).wait_recv()
        att_copy(x_down, part, 0, x_up, 4).start()
        att_copy(x_up, part, 1, x_down, 5).start()

    att_begin(0)

    lax.fori_loop(W_A, W_B, w_pass, 0)

    back.wait_recv()
    att_begin(1)
    att_forward(0)

    lax.fori_loop(W_B, W_C, w_pass, 0)

    att_forward(1)

    lax.fori_loop(W_C, 22, w_pass, 0)

    x_far = ring(x, 2)
    load_w.wait()
    for unit in range(2):
        tok_copy(x_far, unit, x_up, 0).wait_recv()
    for unit in range(2):
        for piece in range(2):
            att_copy(x_far, piece, unit, x_up, 0).wait_recv()

    @pl.loop(0, 4)
    def _(column):
        cols = pl.ds(pl.multiple_of(column * 512, 512), 512)
        projected = jnp.dot(att[...], out_w[:, cols], preferred_element_type=jnp.float32).astype(
            jnp.bfloat16
        )
        tok_cols = tok[:, :, cols].reshape(BLK, 512)
        resid[:, cols] = (tok_cols.astype(jnp.float32) + projected.astype(jnp.float32)).astype(
            jnp.bfloat16
        )
        w_pass(22 + 2 * column, 0)
        w_pass(23 + 2 * column, 0)

    @pl.loop(0, 8)
    def _(tile):
        rows = pl.ds(pl.multiple_of(tile * 64, 64), 64)
        full = resid[rows].astype(jnp.float32)
        scale = lax.rsqrt(jnp.mean(full * full, axis=1, keepdims=True) + 1e-06)
        normed[rows] = (full * scale * mixer_gain[...]).astype(jnp.bfloat16)

    lax.fori_loop(30, 2 * CHIPS, w_pass, 0)

    remote(weights.at[0], weights.at[0], pair_send.at[0], pair_recv.at[0], pair, x).wait_recv()

    def hidden_of(owner):
        rows = pl.ds(pl.multiple_of(owner * ROWS, ROWS), ROWS)
        hidden = jnp.dot(normed[rows], weights[0], preferred_element_type=jnp.float32)
        return jnp.square(jnp.maximum(hidden, 0.0)).astype(jnp.bfloat16)

    def down(hidden, column, width):
        return lax.dot_general(
            hidden,
            weights[1, column : column + width],
            (((1,), (1,)), ((), ())),
            preferred_element_type=jnp.float32,
        )

    wide = D // 2

    def relay_copy(number, to):
        return remote(
            part.at[0, number], relay.at[number], sum_send.at[number], sum_recv.at[number], sp, to
        )

    def final_copy(number, half, to):
        return remote(
            part.at[1 + number, half],
            arrived.at[number, half],
            sum_send.at[2 + number * 2 + half],
            sum_recv.at[2 + number * 2 + half],
            sp,
            to,
        )

    hidden = hidden_of(x_far)
    for half, to in ((0, x_up), (1, x_down)):
        part[0, half] = down(hidden, half * wide, wide).astype(jnp.bfloat16)
        relay_copy(half, to).start()

    near = []
    for number, to in ((0, x_up), (1, x_down)):
        plain = 1 - number
        near.append(hidden_of(to))
        part[1 + number, plain] = down(near[number], plain * wide, wide).astype(jnp.bfloat16)
        final_copy(number, plain, to).start()
    for number, to in ((0, x_up), (1, x_down)):
        added = down(near[number], number * wide, wide)
        relay_copy(number, to).wait_recv()
        part[1 + number, number] = (added + relay[number].astype(jnp.float32)).astype(jnp.bfloat16)
        final_copy(number, number, to).start()

    hidden = hidden_of(x)
    own_rows = pl.ds(pl.multiple_of(x * ROWS, ROWS), ROWS)
    for half in range(2):
        cols = slice(half * wide, (half + 1) * wide)
        total = down(hidden, half * wide, wide) + resid[own_rows, cols].astype(jnp.float32)
        for number in range(2):
            final_copy(number, half, x_up).wait_recv()
            total = total + arrived[number, half].astype(jnp.float32)
        result[:, cols] = total.astype(jnp.bfloat16)

    swap_q.wait_send()
    back.wait_send()
    for copy in swaps:
        copy.wait_send()
    for sem in range(6):
        tok_copy(x, 0, x_up, sem).wait_send()
        for piece in range(2):
            att_copy(x, piece, 0, x_up, sem).wait_send()
    sent_kv = kv.at[pl.ds(0, 28)]
    remote(sent_kv, sent_kv, kv_send.at[0], kv_recv.at[0], y_up, x).wait_send()
    sent_kv = kv.at[pl.ds(0, 32)]
    remote(sent_kv, sent_kv, kv_pair.at[0], kv_recv.at[0], pair, x).wait_send()
    sent_w = weights.at[0, pl.ds(0, 60 * 32)]
    remote(sent_w, sent_w, w_send.at[0], w_recv.at[0, 0], y_up, x).wait_send()
    remote(weights.at[0], weights.at[0], pair_send.at[0], pair_recv.at[0], pair, x).wait_send()
    for number in range(2):
        relay_copy(number, x_up).wait_send()
        for half in range(2):
            final_copy(number, half, x_up).wait_send()


def per_device(
    tokens,
    queries,
    keys,
    values,
    lambdas,
    head_gain,
    out_weight,
    mixer_gain,
    up_weight,
    down_weight,
):
    any_ref = pl.BlockSpec(memory_space=pl.ANY)
    vmem = pl.BlockSpec(memory_space=pltpu.VMEM)
    smem = pl.BlockSpec(memory_space=pltpu.SMEM)
    bf16, f32 = jnp.bfloat16, jnp.float32
    dma = pltpu.SemaphoreType.DMA
    return pl.pallas_call(
        layer_kernel,
        out_shape=jax.ShapeDtypeStruct(tokens.shape, bf16),
        in_specs=[any_ref] * 4 + [smem, vmem, any_ref, vmem, any_ref, any_ref],
        out_specs=vmem,
        scratch_shapes=[
            pltpu.VMEM((64, HALF, 2 * DV), bf16),
            pltpu.VMEM((2, BLK, DV), bf16),
            pltpu.VMEM((BLK, DV), bf16),
            pltpu.VMEM((2, HALF, 2 * DV), bf16),
            pltpu.VMEM((2, 2, DV, BLK), bf16),
            pltpu.VMEM((2, DV + SUMROWS, BLK), bf16),
            pltpu.VMEM((2, BLK, BLK), f32),
            pltpu.VMEM((2, BLK, BLK), f32),
            pltpu.VMEM((2, 2, 1, BLK), f32),
            pltpu.VMEM((2, 2, 1, BLK), f32),
            pltpu.VMEM((2, 2, DV + SUMROWS, BLK), f32),
            pltpu.VMEM((2, D, FFT), bf16),
            pltpu.VMEM((1024, D), bf16),
            pltpu.VMEM((TP, ROWS, D), bf16),
            pltpu.VMEM((BLK, DV), bf16),
            pltpu.VMEM((BLK, 1024), bf16),
            pltpu.VMEM((BLK, D), bf16),
            pltpu.VMEM((BLK, D), bf16),
            pltpu.VMEM((3, 2, ROWS, D // 2), bf16),
            pltpu.VMEM((2, ROWS, D // 2), bf16),
            pltpu.VMEM((2, 2, ROWS, D // 2), bf16),
            dma((13,)),
            dma((1,)),
            dma((8,)),
            dma((2,)),
            dma((1,)),
            dma((1,)),
            dma((64,)),
            dma((1,)),
            dma((2, 32)),
            dma((1,)),
            dma((1,)),
            dma((6,)),
            dma((TP, 2)),
            dma((2,)),
            dma((12,)),
            dma((TP, 4)),
            dma((6,)),
            dma((6,)),
        ],
        compiler_params=pltpu.CompilerParams(
            collective_id=0, has_side_effects=True, vmem_limit_bytes=56 * 1024 * 1024
        ),
    )(
        tokens,
        queries,
        keys,
        values,
        lambdas,
        head_gain.reshape(1, -1),
        out_weight,
        mixer_gain.reshape(1, -1),
        up_weight,
        down_weight.T,
    )


def solution(mesh):
    placed = (
        P(("sp", "tp"), None),
        P("sp", "tp"),
        P("sp", "tp"),
        P("sp", "tp"),
        P("tp"),
        P(),
        P(),
        P(),
        P("sp", "tp"),
        P("tp", "sp"),
    )
    return jax.shard_map(
        per_device, mesh=mesh, in_specs=placed, out_specs=P(("sp", "tp"), None), check_vma=False
    )
```

```python
import jax
import jax.numpy as jnp
from jax import lax
from jax.experimental import pallas as pl
from jax.experimental.pallas import tpu as pltpu
from jax.sharding import PartitionSpec as P

MESH = pl.DeviceIdType.MESH
DQK = 64
DV = 128
BLK = 512
HALF = 256
RING = 4
CHIPS = 16
TP = 4
D = 2048
FFT = 1024
ROWS = 128
SUMROWS = 16
W_NEXT = 22
W_A, W_B, W_C, W_P = 34 - W_NEXT, 22, 24, 24

HERE, LEFT, RIGHT, FAR = 0, 1, 2, 3
FIRST = (HERE, LEFT, RIGHT, HERE, HERE, FAR, HERE, LEFT, LEFT, RIGHT, RIGHT, LEFT, RIGHT, FAR, FAR, FAR)
SECOND = (HERE, HERE, HERE, LEFT, RIGHT, HERE, FAR, LEFT, RIGHT, LEFT, RIGHT, FAR, FAR, LEFT, RIGHT, FAR)

OWN, SWAPPED = 0, 1
KV_KIND = (OWN, SWAPPED, OWN, OWN, OWN, SWAPPED, SWAPPED, SWAPPED, OWN, OWN, SWAPPED, OWN, SWAPPED, SWAPPED, OWN, SWAPPED)
KV_PLACE = (HERE, HERE, HERE, LEFT, RIGHT, HERE, LEFT, RIGHT, LEFT, RIGHT, FAR, FAR, LEFT, RIGHT, FAR, FAR)
KV_MATE = (0, 0, 1, 0, 0, 1, 0, 0, 1, 1, 0, 0, 1, 1, 1, 1)

KV_CODE = tuple(k + 2 * m + 4 * p for k, m, p in zip(KV_KIND, KV_MATE, KV_PLACE))
W_CODE = tuple(f + 4 * s for f, s in zip(FIRST, SECOND))


def pick(index, table):
    value = jnp.int32(0)
    for at, entry in enumerate(table):
        if entry:
            value = value + jnp.where(index == at, entry, 0)
    return value


def shift(place):
    return jnp.where(place == LEFT, 3, jnp.where(place == RIGHT, 1, jnp.where(place == FAR, 2, 0)))


def remote(src, dst, send_sem, recv_sem, sp, tp):
    return pltpu.make_async_remote_copy(
        src_ref=src,
        dst_ref=dst,
        send_sem=send_sem,
        recv_sem=recv_sem,
        device_id=(sp, tp),
        device_id_type=MESH,
    )


def layer_kernel(
    tokens,
    queries,
    keys,
    values,
    lambdas,
    head_gain,
    out_weight,
    mixer_gain,
    up_weight,
    down_weight,
    result,
    kv,
    q_in,
    q_given,
    kv_given,
    q_t,
    v_t,
    scores_a,
    scores_b,
    top,
    run_max,
    acc,
    weights,
    out_w,
    tok,
    stage,
    att,
    resid,
    normed,
    part,
    relay,
    arrived,
    own_sem,
    load_sem,
    swap_sem,
    q_sem,
    kv_send,
    kv_pair,
    kv_recv,
    w_send,
    w_recv,
    pair_send,
    pair_recv,
    tok_send,
    tok_recv,
    back_sem,
    att_send,
    att_recv,
    sum_send,
    sum_recv,
):
    sp = lax.axis_index("sp")
    x = lax.axis_index("tp")
    core = lax.rem(sp, 2)
    chip = sp // 2
    y = lax.rem(chip, RING)
    z = chip // RING
    mirror = 2 * CHIPS - 1 - sp
    pair = chip * 2 + (1 - core)
    side = z // 2
    mate_z = z + 1 - 2 * lax.rem(z, 2)

    def ring(place, step):
        return lax.rem(place + step, RING)

    def at(yy, zz):
        return (zz * RING + yy) * 2 + core

    y_up, y_down = at(ring(y, 1), z), at(ring(y, 3), z)
    z_up, z_down = at(y, ring(z, 1)), at(y, ring(z, 3))
    x_up, x_down = ring(x, 1), ring(x, 3)

    mate, partner = at(y, mate_z), at(y, 3 - z)

    barrier = pltpu.get_barrier_semaphore()
    greeted = [(s, x) for s in (y_up, y_down, z_up, z_down, pair, mirror)]
    greeted += [(sp, x_up), (sp, x_down)]
    for device in greeted:
        pl.semaphore_signal(barrier, inc=1, device_id=device, device_id_type=MESH)

    def lanes(place):
        return pl.ds(pl.multiple_of(place * DV, DV), DV)

    kept, given = lanes(side), lanes(1 - side)
    own_q = pltpu.make_async_copy(queries.at[:, kept], q_in.at[0], own_sem.at[0])
    load_q = pltpu.make_async_copy(queries.at[:, given], q_given, own_sem.at[8])
    swap_q = remote(q_given, q_in.at[1], q_sem.at[0], q_sem.at[1], mirror, x)
    swaps = []
    owns = []
    loads = [load_q]
    for number, (array, half) in enumerate(((keys, pl.ds(0, DV)), (values, pl.ds(DV, DV)))):
        for unit in range(2):
            rows = pl.ds(unit * HALF, HALF)
            place = kv.at[sp * 2 + unit, :, half]
            index = number * 2 + unit
            held = kv_given.at[unit, :, half]
            loads.append(pltpu.make_async_copy(array.at[rows, given], held, own_sem.at[9 + index]))
            swaps.append(
                remote(held, place, swap_sem.at[4 + index], swap_sem.at[index], partner, x)
            )
            owns.append(pltpu.make_async_copy(array.at[rows, kept], place, own_sem.at[1 + index]))
    own_tok = pltpu.make_async_copy(tokens, tok.at[x], own_sem.at[5])
    for copy in loads + owns + [own_q, own_tok]:
        copy.start()

    run_max[...] = jnp.full(run_max.shape, -1e30, jnp.float32)
    acc[...] = jnp.zeros(acc.shape, jnp.float32)
    v_t[...] = jnp.ones(v_t.shape, jnp.bfloat16)
    scores_b[...] = jnp.full(scores_b.shape, -1e30, jnp.float32)
    top[...] = jnp.full(top.shape, -1e30, jnp.float32)

    pl.semaphore_wait(barrier, len(greeted))

    for copy in loads:
        copy.wait()
    for copy in swaps:
        copy.start()
    swap_q.start()

    def tok_copy(source, unit, to, fwd):
        rows = pl.ds(unit * (ROWS // 2), ROWS // 2)
        return remote(
            tok.at[source, rows], tok.at[source, rows], tok_send.at[fwd], tok_recv.at[source, unit], sp, to
        )

    own_w = []
    w_row = chip * 128 + core * 64
    for number, array in enumerate((up_weight, down_weight)):
        own_w.append(
            pltpu.make_async_copy(
                array, weights.at[number, pl.ds(pl.multiple_of(w_row, 64), 64)], own_sem.at[6 + number]
            )
        )
        own_w[-1].start()
    load_w = pltpu.make_async_copy(out_weight, out_w, load_sem.at[0])
    load_w.start()

    for copy in owns:
        copy.wait()

    def item_of(number):
        odd = lax.rem(number, 2)
        code = pick(number // 2, W_CODE)
        first, second = lax.rem(code, 4), code // 4
        y_step = jnp.where(odd == 0, shift(first), shift(second))
        z_step = jnp.where(odd == 0, shift(second), shift(first))
        source = ring(z, z_step) * RING + ring(y, y_step)
        return odd, first, second, source

    def pass_on(number, ref_of, send_sem, recv_of):
        odd, first, second, source = decoded = item_of(number)
        first_up = jnp.where(odd == 0, y_up, z_up)
        first_down = jnp.where(odd == 0, y_down, z_down)
        second_up = jnp.where(odd == 0, z_up, y_up)
        second_down = jnp.where(odd == 0, z_down, y_down)
        at_turn = second == HERE
        at_start = at_turn & (first == HERE)
        halves = (second == FAR) | (at_turn & (first == FAR))

        def copy(unit, to):
            ref = ref_of(odd, source, unit)
            return remote(ref, ref, send_sem, recv_of(odd, source, 0 if unit is None else unit), to, x)

        @pl.when(jnp.logical_not(at_start) & halves)
        def _():
            copy(0, sp).wait_recv()
            copy(1, sp).wait_recv()

        @pl.when(jnp.logical_not(at_start | halves))
        def _():
            copy(None, sp).wait_recv()

        for unit, to, sends in (
            (None, first_up, at_start),
            (None, first_down, at_start),
            (0, first_up, at_turn & (first == LEFT)),
            (1, first_down, at_turn & (first == RIGHT)),
            (None, second_up, at_turn),
            (None, second_down, at_turn),
            (0, second_up, second == LEFT),
            (1, second_down, second == RIGHT),
        ):

            @pl.when(sends)
            def _(unit=unit, to=to):
                copy(unit, to).start()

        return decoded

    def kv_item(number):
        code = pick(number, KV_CODE)
        kind = lax.rem(code, 2)
        by_mate = lax.rem(code // 2, 2)
        place = code // 4
        through = jnp.where(by_mate == 1, mate_z, z)
        source_z = jnp.where(kind == OWN, through, 3 - through)
        return kind, place, by_mate, source_z * RING + ring(y, shift(place))

    def kv_pass(number, item):
        kind, place, by_mate, source = item
        block = source * 2 + core

        def copy(unit, to, send_sem=kv_send.at[0]):
            ref = kv.at[pl.ds(block * 2, 2)] if unit is None else kv.at[block * 2 + unit]
            recv_sem = kv_recv.at[block * 2 + (0 if unit is None else unit)]
            return remote(ref, ref, send_sem, recv_sem, to, x)

        direct = (kind == OWN) | (by_mate == 0)
        swapped_in = (kind == SWAPPED) & (place == HERE) & (by_mate == 0)
        halves = direct & (place == FAR)

        @pl.when(swapped_in)
        def _():
            for copied in swaps:
                copied.wait_recv()

        @pl.when(halves)
        def _():
            copy(0, sp).wait_recv()
            copy(1, sp).wait_recv()

        @pl.when(jnp.logical_not(swapped_in | halves | (number == 0)))
        def _():
            copy(None, sp).wait_recv()

        to_mate = (by_mate == 0) & ((kind == SWAPPED) | (place == HERE))
        for unit, to, sends in (
            (None, y_up, direct & (place == HERE)),
            (None, y_down, direct & (place == HERE)),
            (0, y_up, direct & (place == LEFT)),
            (1, y_down, direct & (place == RIGHT)),
            (None, mate, to_mate),
        ):

            @pl.when(sends)
            def _(unit=unit, to=to):
                copy(unit, to).start()

        copy(None, pair, kv_pair.at[0]).start()

    def w_ref(odd, source, unit):
        row = source * 128 + core * 64
        if unit is None:
            return weights.at[odd, pl.ds(pl.multiple_of(row, 64), 64)]
        return weights.at[odd, pl.ds(pl.multiple_of(row + unit * 32, 32), 32)]

    def w_sem(odd, source, unit):
        return w_recv.at[odd, source * 2 + unit]

    def w_own(odd, to):
        item = w_ref(odd, chip, None)
        remote(item, item, w_send.at[0], w_sem(odd, chip, 0), to, x).start()

    def w_pass(number, carry):
        odd, _, _, source = pass_on(number, w_ref, w_send.at[0], w_sem)
        item = w_ref(odd, source, None)
        remote(item, item, pair_send.at[0], pair_recv.at[0], pair, x).start()
        return carry

    kv_pass(jnp.int32(0), kv_item(jnp.int32(0)))
    for copy in own_w:
        copy.wait()
    for odd in range(2):
        for to in (y_up, y_down, mate):
            w_own(odd, to)
        item = w_ref(odd, chip, None)
        remote(item, item, pair_send.at[0], pair_recv.at[0], pair, x).start()
    own_tok.wait()
    for unit in range(2):
        for number, to in enumerate((x_up, x_down)):
            tok_copy(x, unit, to, unit * 2 + number).start()
    kv_pass(jnp.int32(1), kv_item(jnp.int32(1)))
    for odd in range(2):
        w_own(odd, partner)
    kv_pass(jnp.int32(2), kv_item(jnp.int32(2)))
    own_q.wait()
    swap_q.wait_recv()

    for slot in range(2):
        q_slot = (q_in[slot].astype(jnp.float32) * DQK ** -0.5).T.astype(jnp.bfloat16)
        zero = jnp.zeros((DQK, BLK), jnp.bfloat16)
        q_t[slot, 0, :DQK] = q_slot[:DQK]
        q_t[slot, 0, DQK:] = zero
        q_t[slot, 1, :DQK] = zero
        q_t[slot, 1, DQK:] = q_slot[DQK:]

    scores_of = (scores_a, scores_b)

    def absorb(before, j, weight, new_max, slot):
        shrink = jnp.exp(run_max[slot, j] - new_max)
        acc[slot, j] = acc[slot, j] * shrink + jnp.dot(
            v_t[before], weight, preferred_element_type=jnp.float32
        )
        run_max[slot, j] = new_max

    def softmax(before, j, slot):
        new_max = jnp.maximum(run_max[slot, j], top[before, j])
        weight = jnp.exp(scores_of[before][j] - new_max).astype(jnp.bfloat16)
        return weight, new_max

    def step(now, block, slot, last_slot, masked):
        before = 1 - now
        key = kv[pl.ds(block * 2, 2), :, :DV].reshape(BLK, DV)
        v_t[now, :DV, :] = kv[pl.ds(block * 2, 2), :, DV:].reshape(BLK, DV).T
        for j in range(2):
            scores = jnp.dot(key, q_t[slot, j], preferred_element_type=jnp.float32)
            if masked:
                k_pos = lax.broadcasted_iota(jnp.int32, (BLK, BLK), 0)
                q_pos = lax.broadcasted_iota(jnp.int32, (BLK, BLK), 1)
                scores = jnp.where(k_pos <= q_pos, scores, -1e30)
            scores_of[now][j] = scores
            top[now, j] = jnp.max(scores, axis=0, keepdims=True)
            weight, new_max = softmax(before, j, last_slot)
            absorb(before, j, weight, new_max, last_slot)

    def kv_body(number, carry):
        item = number // 2
        passed = lax.rem(number, 2)
        decoded = kv_item(item)
        block = decoded[3] * 2 + jnp.where(passed == 1, 1 - core, core)

        @pl.when((passed == 0) & (item >= 3))
        def _():
            kv_pass(item, decoded)

        @pl.when(passed == 1)
        def _():
            ref = kv.at[pl.ds(block * 2, 2)]
            remote(ref, ref, kv_send.at[0], kv_recv.at[block * 2], pair, x).wait_recv()

        @pl.when(number >= W_NEXT)
        def _():
            w_pass(number - W_NEXT + 2, 0)

        @pl.when(number == 10)
        def _():
            for unit in range(2):
                tok_copy(x_down, unit, x_up, 0).wait_recv()
                tok_copy(x_up, unit, x_down, 0).wait_recv()
            tok_copy(x_down, 0, x_up, 4).start()
            tok_copy(x_up, 1, x_down, 5).start()

        def slot_body(slot, inner):
            now, last_slot = inner
            q_block = jnp.where(slot == 0, sp, mirror)
            for parity in range(2):
                for masked in (False, True):
                    wanted = (block == q_block) if masked else (block < q_block)

                    @pl.when((now == parity) & wanted)
                    def _(parity=parity, masked=masked):
                        step(parity, block, slot, last_slot, masked)

            done = block <= q_block
            return jnp.where(done, 1 - now, now), jnp.where(done, slot, last_slot)

        return lax.fori_loop(0, 2, slot_body, carry)

    _, last_slot = lax.fori_loop(0, 2 * CHIPS, kv_body, (jnp.int32(0), jnp.int32(0)))
    for j in range(2):
        weight, new_max = softmax(0, j, last_slot)
        absorb(0, j, weight, new_max, last_slot)

    def att_lanes(source, part):
        head = side if part == 0 else 1 - side
        return pl.ds(pl.multiple_of((source * 2 + head) * DV, DV), DV)

    back = remote(
        stage, att.at[:, att_lanes(x, 0)], back_sem.at[0], back_sem.at[1], mirror, x
    )

    for slot in (1, 0):
        map_1 = acc[slot, 0, :DV] / acc[slot, 0, DV : DV + 1]
        map_2 = acc[slot, 1, :DV] / acc[slot, 1, DV : DV + 1]
        lam = jnp.where(side == 0, lambdas[0], lambdas[1])
        differ = map_1 - lam * map_2
        spread = lax.rsqrt(jnp.mean(differ * differ, axis=0, keepdims=True) + 1e-06)
        attended = ((differ * spread).T * head_gain[...]).astype(jnp.bfloat16)
        if slot == 1:
            stage[...] = attended
            back.start()
        else:
            att[:, att_lanes(x, 0)] = attended

    def att_copy(source, part, unit, to, sem):
        place = att.at[pl.ds(unit * HALF, HALF), att_lanes(source, part)]
        return remote(
            place, place, att_send.at[part * 6 + sem], att_recv.at[source, part * 2 + unit], sp, to
        )

    def att_begin(part):
        for unit in range(2):
            for number, to in enumerate((x_up, x_down)):
                att_copy(x, part, unit, to, unit * 2 + number).start()

    def att_forward(part):
        for unit in range(2):
            att_copy(x_down, part, unit, x_up, 0).wait_recv()
            att_copy(x_up, part, unit, x_down, 0).wait_recv()
        att_copy(x_down, part, 0, x_up, 4).start()
        att_copy(x_up, part, 1, x_down, 5).start()

    att_begin(0)

    lax.fori_loop(W_A, W_B, w_pass, 0)

    back.wait_recv()
    att_begin(1)
    att_forward(0)

    lax.fori_loop(W_B, W_C, w_pass, 0)

    att_forward(1)

    lax.fori_loop(W_C, W_P, w_pass, 0)

    x_far = ring(x, 2)
    load_w.wait()
    for unit in range(2):
        tok_copy(x_far, unit, x_up, 0).wait_recv()
    for unit in range(2):
        for piece in range(2):
            att_copy(x_far, piece, unit, x_up, 0).wait_recv()

    @pl.loop(0, 4)
    def _(column):
        cols = pl.ds(pl.multiple_of(column * 512, 512), 512)
        projected = jnp.dot(att[...], out_w[:, cols], preferred_element_type=jnp.float32).astype(
            jnp.bfloat16
        )
        tok_cols = tok[:, :, cols].reshape(BLK, 512)
        resid[:, cols] = (tok_cols.astype(jnp.float32) + projected.astype(jnp.float32)).astype(
            jnp.bfloat16
        )
        w_pass(W_P + 2 * column, 0)
        w_pass(W_P + 1 + 2 * column, 0)

    @pl.loop(0, 8)
    def _(tile):
        rows = pl.ds(pl.multiple_of(tile * 64, 64), 64)
        full = resid[rows].astype(jnp.float32)
        scale = lax.rsqrt(jnp.mean(full * full, axis=1, keepdims=True) + 1e-06)
        normed[rows] = (full * scale * mixer_gain[...]).astype(jnp.bfloat16)

    lax.fori_loop(W_P + 8, 2 * CHIPS, w_pass, 0)

    remote(weights.at[0], weights.at[0], pair_send.at[0], pair_recv.at[0], pair, x).wait_recv()

    def hidden_of(owner):
        rows = pl.ds(pl.multiple_of(owner * ROWS, ROWS), ROWS)
        hidden = jnp.dot(normed[rows], weights[0], preferred_element_type=jnp.float32)
        return jnp.square(jnp.maximum(hidden, 0.0)).astype(jnp.bfloat16)

    def down(hidden, column, width):
        return lax.dot_general(
            hidden,
            weights[1, column : column + width],
            (((1,), (1,)), ((), ())),
            preferred_element_type=jnp.float32,
        )

    wide = D // 2

    def relay_copy(number, to):
        return remote(
            part.at[0, number], relay.at[number], sum_send.at[number], sum_recv.at[number], sp, to
        )

    def final_copy(number, half, to):
        return remote(
            part.at[1 + number, half],
            arrived.at[number, half],
            sum_send.at[2 + number * 2 + half],
            sum_recv.at[2 + number * 2 + half],
            sp,
            to,
        )

    hidden = hidden_of(x_far)
    for half, to in ((0, x_up), (1, x_down)):
        part[0, half] = down(hidden, half * wide, wide).astype(jnp.bfloat16)
        relay_copy(half, to).start()

    near = []
    for number, to in ((0, x_up), (1, x_down)):
        plain = 1 - number
        near.append(hidden_of(to))
        part[1 + number, plain] = down(near[number], plain * wide, wide).astype(jnp.bfloat16)
        final_copy(number, plain, to).start()
    for number, to in ((0, x_up), (1, x_down)):
        added = down(near[number], number * wide, wide)
        relay_copy(number, to).wait_recv()
        part[1 + number, number] = (added + relay[number].astype(jnp.float32)).astype(jnp.bfloat16)
        final_copy(number, number, to).start()

    hidden = hidden_of(x)
    own_rows = pl.ds(pl.multiple_of(x * ROWS, ROWS), ROWS)
    for half in range(2):
        cols = slice(half * wide, (half + 1) * wide)
        total = down(hidden, half * wide, wide) + resid[own_rows, cols].astype(jnp.float32)
        for number in range(2):
            final_copy(number, half, x_up).wait_recv()
            total = total + arrived[number, half].astype(jnp.float32)
        result[:, cols] = total.astype(jnp.bfloat16)

    swap_q.wait_send()
    back.wait_send()
    for copy in swaps:
        copy.wait_send()
    for sem in range(6):
        tok_copy(x, 0, x_up, sem).wait_send()
        for piece in range(2):
            att_copy(x, piece, 0, x_up, sem).wait_send()
    sent_kv = kv.at[pl.ds(0, 28)]
    remote(sent_kv, sent_kv, kv_send.at[0], kv_recv.at[0], y_up, x).wait_send()
    sent_kv = kv.at[pl.ds(0, 32)]
    remote(sent_kv, sent_kv, kv_pair.at[0], kv_recv.at[0], pair, x).wait_send()
    sent_w = weights.at[0, pl.ds(0, 60 * 32)]
    remote(sent_w, sent_w, w_send.at[0], w_recv.at[0, 0], y_up, x).wait_send()
    remote(weights.at[0], weights.at[0], pair_send.at[0], pair_recv.at[0], pair, x).wait_send()
    for number in range(2):
        relay_copy(number, x_up).wait_send()
        for half in range(2):
            final_copy(number, half, x_up).wait_send()


def per_device(
    tokens,
    queries,
    keys,
    values,
    lambdas,
    head_gain,
    out_weight,
    mixer_gain,
    up_weight,
    down_weight,
):
    any_ref = pl.BlockSpec(memory_space=pl.ANY)
    vmem = pl.BlockSpec(memory_space=pltpu.VMEM)
    smem = pl.BlockSpec(memory_space=pltpu.SMEM)
    bf16, f32 = jnp.bfloat16, jnp.float32
    dma = pltpu.SemaphoreType.DMA
    return pl.pallas_call(
        layer_kernel,
        out_shape=jax.ShapeDtypeStruct(tokens.shape, bf16),
        in_specs=[any_ref] * 4 + [smem, vmem, any_ref, vmem, any_ref, any_ref],
        out_specs=vmem,
        scratch_shapes=[
            pltpu.VMEM((64, HALF, 2 * DV), bf16),
            pltpu.VMEM((2, BLK, DV), bf16),
            pltpu.VMEM((BLK, DV), bf16),
            pltpu.VMEM((2, HALF, 2 * DV), bf16),
            pltpu.VMEM((2, 2, DV, BLK), bf16),
            pltpu.VMEM((2, DV + SUMROWS, BLK), bf16),
            pltpu.VMEM((2, BLK, BLK), f32),
            pltpu.VMEM((2, BLK, BLK), f32),
            pltpu.VMEM((2, 2, 1, BLK), f32),
            pltpu.VMEM((2, 2, 1, BLK), f32),
            pltpu.VMEM((2, 2, DV + SUMROWS, BLK), f32),
            pltpu.VMEM((2, D, FFT), bf16),
            pltpu.VMEM((1024, D), bf16),
            pltpu.VMEM((TP, ROWS, D), bf16),
            pltpu.VMEM((BLK, DV), bf16),
            pltpu.VMEM((BLK, 1024), bf16),
            pltpu.VMEM((BLK, D), bf16),
            pltpu.VMEM((BLK, D), bf16),
            pltpu.VMEM((3, 2, ROWS, D // 2), bf16),
            pltpu.VMEM((2, ROWS, D // 2), bf16),
            pltpu.VMEM((2, 2, ROWS, D // 2), bf16),
            dma((13,)),
            dma((1,)),
            dma((8,)),
            dma((2,)),
            dma((1,)),
            dma((1,)),
            dma((64,)),
            dma((1,)),
            dma((2, 32)),
            dma((1,)),
            dma((1,)),
            dma((6,)),
            dma((TP, 2)),
            dma((2,)),
            dma((12,)),
            dma((TP, 4)),
            dma((6,)),
            dma((6,)),
        ],
        compiler_params=pltpu.CompilerParams(
            collective_id=0, has_side_effects=True, vmem_limit_bytes=56 * 1024 * 1024
        ),
    )(
        tokens,
        queries,
        keys,
        values,
        lambdas,
        head_gain.reshape(1, -1),
        out_weight,
        mixer_gain.reshape(1, -1),
        up_weight,
        down_weight.T,
    )


def solution(mesh):
    placed = (
        P(("sp", "tp"), None),
        P("sp", "tp"),
        P("sp", "tp"),
        P("sp", "tp"),
        P("tp"),
        P(),
        P(),
        P(),
        P("sp", "tp"),
        P("tp", "sp"),
    )
    return jax.shard_map(
        per_device, mesh=mesh, in_specs=placed, out_specs=P(("sp", "tp"), None), check_vma=False
    )
```
